128 devices in a mesh: sp: 16 (over z, y), dp: 8 (over x, core).
Axes of the slice: x: 4, y: 4, z: 4, core: 2. Of those that a mesh axis runs over, the one named last changes fastest.
Arguments:
- queries: bfloat16 [8, 2048, 3072], P('dp', 'sp'), may hold values from -20 to 20
- kv_latent: bfloat16 [8, 2048, 256], P('dp', 'sp'), may hold values from -60 to 60
- rope_key: bfloat16 [8, 2048, 32], P('dp', 'sp'), may hold values from -20 to 20
- latent_norm_gain: float32 [256], replicated, may hold values from 0.1 to 1.9
- key_up_weight: bfloat16 [256, 2048], replicated, may hold values from -0.375 to 0.375
- value_up_weight: bfloat16 [256, 2048], replicated, may hold values from -0.375 to 0.375
- out_proj: bfloat16 [2048, 2048], replicated, may hold values from -0.125 to 0.125
- residual: bfloat16 [8, 2048, 2048], P('dp', 'sp'), may hold values from -0.59765625 to 0.59765625
- ffn_gain: float32 [2048], replicated, may hold values from 0.1 to 1.9
- routes: int32 [8, 2048, 2], P('dp', 'sp'), may hold values from 0 to 127, all different within a row; in each aligned block of 128 rows (0 to 127, 128 to 255, ..., all dimensions but the last counted through in order) at most 4 rows name the same one
- route_weights: float32 [8, 2048, 2], P('dp', 'sp'), may hold values from 0.1 to 1
- expert_gate: bfloat16 [128, 2048, 1024], P(('sp', 'dp')), may hold values from -1.3258252 to 1.3258252
- expert_up: bfloat16 [128, 2048, 1024], P(('sp', 'dp')), may hold values from -1.3258252 to 1.3258252
- expert_down: bfloat16 [128, 1024, 2048], P(('sp', 'dp')), may hold values from -0.1875 to 0.1875
Outputs:
- normed_rows: bfloat16 [8, 2048, 2048], P('dp', 'sp')
- layer_out: bfloat16 [8, 2048, 2048], P('dp', 'sp')
The draws below stay inside these ranges and needn't reach their ends.
Inputs may be any that keep to these rules, and one draw needn't show every extreme that they name: `routes`: each token names 2 different experts. Among the tokens of one device no expert is named more than 4 times, and in some devices' tokens an expert is named exactly 4 times.
All inputs are finite; a program needn't handle non-finite values.
Results may differ from the reference program's by a relative error of at most 0.012.
The reference program's roundings to bfloat16 on the way count: a program that leaves them out, or rounds other values in their place, can miss the bound.
Values may be sent and summed in bfloat16 or wider, within the bound.
No kernel may reach another device: no remote copies, remote signals or barrier semaphores. Data moves between devices by JAX's collectives and lax.ppermute only.
A program may use at most 128 MiB of HBM per device.

```python
import math
import jax
import jax.numpy as jnp
import numpy as np
from jax import lax

D = 2048
HEAD_COUNT = 32
PLAIN_HEAD_SIZE = 64
ROTARY_SIZE = 32
VALUE_HEAD_SIZE = 64
LATENT_WIDTH = 256
FF = 1024
TOPK = 2
GRID_W = 64
TOK_DEV = 128
SEQUENCE_LENGTH = 2048
SEQUENCE_COUNT = 8
EXPERTS = 128
CAP = 4


def draw_rope_key(key, part):
    child_random_key = jax.random.fold_in(key, 3)
    return jnp.clip(jax.random.normal(child_random_key, (SEQUENCE_COUNT, SEQUENCE_LENGTH, ROTARY_SIZE), jnp.float32), -6.0, 6.0).astype(jnp.bfloat16)


def draw_queries(key, part):
    child_random_key = jax.random.fold_in(key, 5)
    shape = (SEQUENCE_COUNT, SEQUENCE_LENGTH, HEAD_COUNT, PLAIN_HEAD_SIZE + ROTARY_SIZE)
    starting_random = jnp.clip(2.0 * jax.random.normal(child_random_key, shape, jnp.float32), -12.0, 12.0)
    return starting_random.reshape(SEQUENCE_COUNT, SEQUENCE_LENGTH, HEAD_COUNT * (PLAIN_HEAD_SIZE + ROTARY_SIZE)).astype(jnp.bfloat16)


def draw_kv_latent(key, part):
    child_random_key = jax.random.fold_in(key, 9)
    starting_random = jnp.clip(jax.random.normal(child_random_key, (SEQUENCE_COUNT, SEQUENCE_LENGTH, LATENT_WIDTH), jnp.float32), -6.0, 6.0)
    return starting_random.astype(jnp.bfloat16)


def expert_matrix(key, salt):
    child_random_key = jax.random.fold_in(key, salt)
    starting_random = jnp.clip(jax.random.normal(child_random_key, (EXPERTS, D, FF), jnp.float32), -6.0, 6.0) * D ** (-0.5)
    return starting_random.astype(jnp.bfloat16)


def draw_expert_gate(key, part):
    return expert_matrix(key, 21)


def draw_expert_up(key, part):
    return expert_matrix(key, 23)


def block_levels(key, dims, pieces, low, largest):
    factor_of = 1.0
    for axis_at, shards_of in pieces:
        heights = jax.random.uniform(jax.random.fold_in(jax.random.fold_in(key, 6), axis_at), (shards_of,), jnp.float32, low / len(pieces), largest / len(pieces))
        factor_of = factor_of * jnp.repeat(jnp.exp(heights), dims[axis_at] // shards_of).reshape((-1,) + (1,) * (len(dims) - 1 - axis_at))
    return factor_of


def deal_out(rng, own, number, rows, count, top, reach, lean):
    ranking = jax.random.permutation(rng, count)
    packed, usual = shares(count, rows * top, reach, lean, True), shares(count, rows * top, reach, lean, False)
    places = jnp.arange(count)

    def named(lengths, offset_by):
        used = int((lengths > 0).sum())
        fixed = max(1, used // 4)
        moved = fixed + (places - fixed + offset_by * (used - fixed)) % max(1, count - fixed)
        return jnp.zeros((count,), jnp.int32).at[ranking[jnp.where(places < fixed, places, moved)]].set(jnp.asarray(lengths, jnp.int32))

    lengths = jnp.where(number % 4 == 0, named(packed, number // 4), named(usual, number - number // 4 - 1))
    mixed = jax.random.permutation(jax.random.fold_in(own, 3), count)
    donor, taker = mixed[0:count // 2 * 2:2], mixed[1:count // 2 * 2:2]
    slack = jnp.minimum(lengths[donor] - 1, reach - lengths[taker]) // 2
    slack = jnp.where((donor == ranking[0]) | (taker == ranking[0]) | (lengths[taker] == 0), 0, jnp.maximum(slack, 0))
    moved = jax.random.randint(jax.random.fold_in(own, 4), (count // 2,), 0, 1 << 20) % (slack + 1)
    lengths = lengths.at[donor].add(-moved).at[taker].add(moved)
    labels = jnp.searchsorted(jnp.cumsum(lengths), jnp.arange(rows * top), side="right").astype(jnp.int32)
    grid = labels.reshape(top, rows).T
    grid = grid[jax.random.permutation(jax.random.fold_in(own, 1), rows)]
    offset_by = jax.random.randint(jax.random.fold_in(own, 2), (rows, 1), 0, top)
    return jnp.take_along_axis(grid, (jnp.arange(top)[None, :] + offset_by) % top, axis=1)


def shares(count, total, bound, slope, full):
    loads = [(1 << 20) // math.isqrt(grade ** slope) + 1 for grade in range(1, count + 1)]
    largest = bound if full else min(bound, max(-(-total // count), total * loads[0] // sum(loads)))
    least = 1 if total - largest >= count - 1 else 0
    given, rest = [largest] + [least] * (count - 1), total - largest - least * (count - 1)
    while rest > 0:
        candidates = [i for i in range(1, count) if given[i] < largest] or [i for i in range(1, count) if given[i] < bound]
        whole, budget = sum([loads[i] for i in candidates]), rest
        for i in candidates:
            extra = min(bound - given[i], max(1, budget * loads[i] // whole), rest)
            given[i] = given[i] + extra
            rest = rest - extra
    return np.array(given)


def bell_draw(rng, dims, width, reach, shards=(), kind=jnp.bfloat16):
    values = jax.random.normal(rng, dims, jnp.float32) * width
    if len(shards) > 0:
        values = block_levels(rng, dims, shards, -0.22, 0.18) * values
    return jnp.clip(values, min=-reach, max=reach).astype(kind)


def setup_inputs(seed: int = 0) -> dict:
    seeds = jax.random.split(jax.random.key(seed), 15)
    queries = draw_queries(jax.random.fold_in(seeds[14], 71), 0)
    kv_latent = draw_kv_latent(jax.random.fold_in(seeds[14], 71), 0)
    rope_key = draw_rope_key(jax.random.fold_in(seeds[14], 71), 0)
    latent_norm_gain = jnp.clip(1.0 + 0.18 * jax.random.normal(seeds[3], (LATENT_WIDTH,), jnp.float32), 0.1, 1.9)
    key_up_weight = bell_draw(seeds[4], (LATENT_WIDTH, HEAD_COUNT * PLAIN_HEAD_SIZE), LATENT_WIDTH ** -0.5, 0.375)
    value_up_weight = bell_draw(seeds[5], (LATENT_WIDTH, HEAD_COUNT * VALUE_HEAD_SIZE), LATENT_WIDTH ** -0.5, 0.375)
    out_proj = bell_draw(seeds[6], (HEAD_COUNT * VALUE_HEAD_SIZE, D), (HEAD_COUNT * VALUE_HEAD_SIZE) ** -0.5, 0.125)
    residual = bell_draw(seeds[7], (SEQUENCE_COUNT, SEQUENCE_LENGTH, D), 0.1, 0.59765625, ((0, 8), (1, 16)))
    ffn_gain = jnp.clip(1.0 + 0.18 * jax.random.normal(seeds[8], (D,), jnp.float32), 0.1, 1.9)
    routes_keys = jax.random.split(jax.random.fold_in(seeds[9], 1), SEQUENCE_COUNT * SEQUENCE_LENGTH // TOK_DEV)
    routes_turns = jax.random.permutation(jax.random.fold_in(seeds[9], 3), SEQUENCE_COUNT * SEQUENCE_LENGTH // TOK_DEV)
    routes = jax.vmap(lambda own, number: deal_out(jax.random.fold_in(seeds[9], 2), own, number, TOK_DEV, EXPERTS, TOPK, CAP, 2))(routes_keys, routes_turns).reshape((SEQUENCE_COUNT, SEQUENCE_LENGTH, TOPK))
    route_weights = jnp.clip(jnp.exp(math.log(1.0) - 2.3025851 * jax.random.uniform(seeds[10], (SEQUENCE_COUNT, SEQUENCE_LENGTH, TOPK), jnp.float32) ** block_levels(seeds[10], (SEQUENCE_COUNT, SEQUENCE_LENGTH, TOPK), ((0, 8), (1, 16)), -0.2, 0.2)), 0.1, 1.0)
    expert_gate = draw_expert_gate(jax.random.fold_in(seeds[14], 71), 0)
    expert_up = draw_expert_up(jax.random.fold_in(seeds[14], 71), 0)
    expert_down = bell_draw(seeds[13], (EXPERTS, FF, D), FF ** -0.5, 0.1875, ((0, 128),))
    return {"queries": queries, "kv_latent": kv_latent, "rope_key": rope_key, "latent_norm_gain": latent_norm_gain, "key_up_weight": key_up_weight, "value_up_weight": value_up_weight, "out_proj": out_proj, "residual": residual, "ffn_gain": ffn_gain, "routes": routes, "route_weights": route_weights, "expert_gate": expert_gate, "expert_up": expert_up, "expert_down": expert_down}


eps_norm = 1e-06
rope_base = 10000.0
clamp_limit = 7.0
glu_alpha = 1.702

def rope_tables(positions):
    grid_row = (positions // GRID_W).astype(jnp.float32)
    grid_col = (positions % GRID_W).astype(jnp.float32)
    quarter = ROTARY_SIZE // 4
    frequency = rope_base ** (-(2.0 * jnp.arange(quarter, dtype=jnp.float32)) / (ROTARY_SIZE // 2))
    angles = jnp.concatenate([grid_row[:, None] * frequency[None, :], grid_col[:, None] * frequency[None, :]], axis=1)
    return (jnp.cos(angles), jnp.sin(angles))

def rotate(entries, cosine_table, sine_table):
    pair_view = entries.reshape(entries.shape[:-1] + (entries.shape[-1] // 2, 2))
    first_half = pair_view[..., 0]
    second_half = pair_view[..., 1]
    turned = jnp.stack([first_half * cosine_table - second_half * sine_table, first_half * sine_table + second_half * cosine_table], axis=-1)
    return turned.reshape(entries.shape)

def rms_scale(entries, gain_vec):
    floats = entries.astype(jnp.float32)
    return floats * lax.rsqrt(lax.optimization_barrier(jnp.mean(floats * floats, axis=-1, keepdims=True)) + eps_norm) * gain_vec.astype(jnp.float32)

def clamped_unit(gate_pre, up_pre):
    gate_cut = jnp.minimum(gate_pre, clamp_limit)
    up_cut = jnp.clip(up_pre, -clamp_limit, clamp_limit)
    return gate_cut * jax.nn.sigmoid(glu_alpha * gate_cut) * (up_cut + 1.0)

def expert_rows(rows, gate_w, up_w, down_w):
    gate_pre = jnp.dot(rows, gate_w, preferred_element_type=jnp.float32)
    up_pre = jnp.dot(rows, up_w, preferred_element_type=jnp.float32)
    hidden = clamped_unit(gate_pre, up_pre).astype(jnp.bfloat16)
    return jnp.dot(hidden, down_w, preferred_element_type=jnp.float32).astype(jnp.bfloat16)

def attend_sequence(query_rows, key_row_list, value_per_head):
    token_length = query_rows.shape[0]
    block_row_count = min(512, token_length)
    blocks = query_rows.reshape(token_length // block_row_count, block_row_count, query_rows.shape[1], query_rows.shape[2])
    key_single_float = key_row_list.astype(jnp.float32)
    latent_single_float = key_single_float[:, :LATENT_WIDTH]
    value_float = value_per_head.astype(jnp.float32)

    def one_block(query_block):
        scores = jnp.einsum('qhd,kd->hqk', query_block.astype(jnp.float32), key_single_float)
        highest = lax.optimization_barrier(jnp.max(scores, axis=-1, keepdims=True))
        weights = jnp.exp(scores - highest)
        weights_brain_float = (weights / lax.optimization_barrier(jnp.sum(weights, axis=-1, keepdims=True))).astype(jnp.bfloat16)
        context = jnp.einsum('nef,fg->eng', weights_brain_float.astype(jnp.float32), latent_single_float).astype(jnp.bfloat16)
        return jnp.einsum('qhc,chv->qhv', context.astype(jnp.float32), value_float).astype(jnp.bfloat16)
    result = lax.map(one_block, blocks)
    return result.reshape(token_length, query_rows.shape[1] * VALUE_HEAD_SIZE)

def route_sum(normed, flat_expert, flat_weight, expert_gate, expert_up, expert_down):
    count_rows = normed.shape[0]
    assign_count = flat_expert.shape[0]
    block_row_count = 128
    sort_order = jnp.argsort(flat_expert, stable=True).astype(jnp.int32)
    sorted_expert = flat_expert[sort_order]
    counts = jnp.bincount(flat_expert, length=EXPERTS).astype(jnp.int32)
    starts = (jnp.cumsum(counts) - counts).astype(jnp.int32)
    padded = ((counts + block_row_count - 1) // block_row_count * block_row_count).astype(jnp.int32)
    pad_ends = jnp.cumsum(padded).astype(jnp.int32)
    pad_starts = (pad_ends - padded).astype(jnp.int32)
    slot_index = (pad_starts[sorted_expert] + jnp.arange(assign_count, dtype=jnp.int32) - starts[sorted_expert]).astype(jnp.int32)
    block_count = (assign_count + EXPERTS * (block_row_count - 1)) // block_row_count + 1
    slot_total = block_count * block_row_count
    slot_token = jnp.full((slot_total,), count_rows, jnp.int32).at[slot_index].set((sort_order // TOPK).astype(jnp.int32))
    slot_weight = jnp.zeros((slot_total,), jnp.float32).at[slot_index].set(flat_weight[sort_order].astype(jnp.float32))
    block_starts = jnp.arange(block_count, dtype=jnp.int32) * block_row_count
    block_expert = jnp.minimum(jnp.searchsorted(pad_ends, block_starts, side='right'), EXPERTS - 1).astype(jnp.int32)
    padded_rows = jnp.concatenate([normed, jnp.zeros((1, normed.shape[1]), normed.dtype)], axis=0)

    def one_block(pair):
        tokens, expert = pair
        rows = padded_rows[tokens]
        return expert_rows(rows, expert_gate[expert], expert_up[expert], expert_down[expert]).astype(jnp.float32)
    outputs = lax.map(one_block, (slot_token.reshape(block_count, block_row_count), block_expert))
    outputs = outputs.reshape(slot_total, normed.shape[1]) * slot_weight[:, None]
    return jax.ops.segment_sum(outputs, slot_token, num_segments=count_rows + 1)[:count_rows]

def reference(queries, kv_latent, rope_key, latent_norm_gain, key_up_weight, value_up_weight, out_proj, residual, ffn_gain, routes, route_weights, expert_gate, expert_up, expert_down):
    positions = jnp.arange(SEQUENCE_LENGTH, dtype=jnp.int32)
    cosine_table, sine_table = rope_tables(positions)
    score_scale = (PLAIN_HEAD_SIZE + ROTARY_SIZE) ** (-0.5)
    query_float = queries.astype(jnp.float32).reshape(SEQUENCE_COUNT, SEQUENCE_LENGTH, HEAD_COUNT, PLAIN_HEAD_SIZE + ROTARY_SIZE)
    query_turned = rotate(query_float[..., PLAIN_HEAD_SIZE:], cosine_table[None, :, None, :], sine_table[None, :, None, :])
    q_ready = (jnp.concatenate([query_float[..., :PLAIN_HEAD_SIZE], query_turned], axis=-1) * score_scale).astype(jnp.bfloat16)
    key_turned = rotate(rope_key.astype(jnp.float32), cosine_table[None], sine_table[None]).astype(jnp.bfloat16)
    latent = rms_scale(kv_latent, latent_norm_gain).astype(jnp.bfloat16)
    key_per_head = key_up_weight.astype(jnp.float32).reshape(LATENT_WIDTH, HEAD_COUNT, PLAIN_HEAD_SIZE)
    value_per_head = value_up_weight.reshape(LATENT_WIDTH, HEAD_COUNT, VALUE_HEAD_SIZE)
    key_row_list = jnp.concatenate([latent, key_turned], axis=-1)

    def per_sequence(pair):
        q_seq, key_seq = pair
        q_latent = jnp.einsum('qhn,chn->qhc', q_seq[..., :PLAIN_HEAD_SIZE].astype(jnp.float32), key_per_head).astype(jnp.bfloat16)
        query_complete = jnp.concatenate([q_latent, q_seq[..., PLAIN_HEAD_SIZE:]], axis=-1)
        return attend_sequence(query_complete, key_seq, value_per_head)
    heads_out = lax.map(per_sequence, (q_ready, key_row_list))
    mixed = residual.reshape(SEQUENCE_COUNT * SEQUENCE_LENGTH, D).astype(jnp.float32) + jnp.dot(heads_out.reshape(SEQUENCE_COUNT * SEQUENCE_LENGTH, HEAD_COUNT * VALUE_HEAD_SIZE), out_proj, preferred_element_type=jnp.float32)
    normed = rms_scale(mixed, ffn_gain).astype(jnp.bfloat16)
    routed = route_sum(normed, routes.reshape(-1).astype(jnp.int32), route_weights.reshape(-1), expert_gate, expert_up, expert_down)
    layer_out = (mixed + routed).astype(jnp.bfloat16)
    return (normed.reshape(SEQUENCE_COUNT, SEQUENCE_LENGTH, D), layer_out.reshape(SEQUENCE_COUNT, SEQUENCE_LENGTH, D))
```

```python
import numpy as np
import jax
import jax.numpy as jnp
from jax import lax
from jax.experimental import pallas as pl
from jax.experimental.pallas import tpu as pltpu
from jax.sharding import PartitionSpec as P

D = 2048
HEADS = 32
PLAIN = 64
ROT = 32
QK = PLAIN + ROT
LAT = 256
TOPK = 2
GRID_W = 64
FF = 1024
CAP = 4
GROUP = 4
EPS = 1e-06
CLAMP = 7.0
ALPHA = 1.702
LOG2E = 1.4426950408889634
BF = jnp.bfloat16
F32 = jnp.float32


def lane_tables(positions, lanes):
    lane = np.arange(lanes)
    if lanes == ROT:
        entry, plain = lane, np.zeros(lanes, bool)
    else:
        entry, plain = lane % QK - PLAIN, lane % QK < PLAIN
    pair = np.where(plain, 0, entry // 2)
    quarter = ROT // 4
    freq = (10000.0 ** (-(2.0 * (pair % quarter)) / (ROT // 2))).astype(np.float32)
    by_row = pair < quarter
    sign = np.where(plain, 0.0, np.where(entry % 2 == 0, -1.0, 1.0)).astype(np.float32)
    row = (positions // GRID_W).astype(F32)[:, None]
    col = (positions % GRID_W).astype(F32)[:, None]
    angle = jnp.where(by_row[None], row, col) * freq[None]
    cosine = jnp.where(plain[None], 1.0, jnp.cos(angle))
    return cosine, jnp.sin(angle) * sign[None]


def turn(x, cosine, sine):
    lanes = x.shape[-1]
    lane = lax.broadcasted_iota(jnp.int32, x.shape, 1)
    swapped = jnp.where(
        lane % 2 == 0, pltpu.roll(x, lanes - 1, 1), pltpu.roll(x, 1, 1)
    )
    return x * cosine + swapped * sine


def key_kernel(lat_ref, rope_ref, gain_ref, cos_ref, sin_ref, out_ref):
    lat = lat_ref[...].astype(F32)
    ms = jnp.mean(lat * lat, axis=-1, keepdims=True)
    latent = (lat * lax.rsqrt(ms + EPS) * gain_ref[...]).astype(BF)
    rope = rope_ref[...].astype(F32)
    wide = jnp.concatenate([rope] * 4, axis=1)
    cw = jnp.concatenate([cos_ref[...]] * 4, axis=1)
    sw = jnp.concatenate([sin_ref[...]] * 4, axis=1)
    turned = turn(wide, cw, sw)[:, :ROT].astype(BF)
    for i in range(out_ref.shape[0]):
        out_ref[i, :, :LAT] = latent
        out_ref[i, :, LAT:] = turned


def route_kernel(col_ref, row_ref, bcol_ref, brow_ref):
    n = col_ref.shape[0]
    sub = lax.broadcasted_iota(jnp.int32, (n, n), 0)
    lane = lax.broadcasted_iota(jnp.int32, (n, n), 1)
    e_c = [col_ref[:, k : k + 1] for k in range(2)]
    e_r = [row_ref[k : k + 1, :] for k in range(2)]
    same00 = e_c[0] == e_r[0]
    same11 = e_c[1] == e_r[1]
    one = lambda m: jnp.where(m, 1.0, 0.0)
    r0 = jnp.sum(one(same00 & (lane < sub)), axis=1, keepdims=True)
    r1 = jnp.sum(one(same11 & (lane < sub)), axis=1, keepdims=True) + jnp.sum(
        one(e_c[1] == e_r[0]), axis=1, keepdims=True
    )
    bcol_ref[:, 0:1] = e_c[0] * 8 + r0.astype(jnp.int32)
    bcol_ref[:, 1:2] = e_c[1] * 8 + r1.astype(jnp.int32)
    s0 = jnp.sum(one(same00 & (sub < lane)), axis=0, keepdims=True)
    s1 = jnp.sum(one(same11 & (sub < lane)), axis=0, keepdims=True) + jnp.sum(
        one(e_c[0] == e_r[1]), axis=0, keepdims=True
    )
    brow_ref[0:1, :] = e_r[0] * 8 + s0.astype(jnp.int32)
    brow_ref[1:2, :] = e_r[1] * 8 + s1.astype(jnp.int32)


def dot(a, b, dims):
    return lax.dot_general(a, b, (dims, ((), ())), preferred_element_type=F32)


def attend_kernel(
    q_ref, cos_ref, sin_ref, keys_ref, ku_ref, vu_ref, wo_ref, res_ref, gain_ref, brow_ref,
    mixed_ref, normed_ref, out_ref,
    klt_ref, qs_ref, acc_ref,
):
    g = pl.program_id(0)
    toks = q_ref.shape[0]

    @pl.when(g == 0)
    def _():
        klt_ref[...] = keys_ref[:, :LAT].T
        acc_ref[...] = res_ref[...].astype(F32)

    q = q_ref[...].astype(F32)
    qr = turn(q, cos_ref[...], sin_ref[...]) * (QK ** -0.5)
    q_ready = qr.astype(BF)
    q_rope = (qr * LOG2E).astype(BF)
    for j in range(GROUP):
        rows = slice(j * toks, (j + 1) * toks)
        qn = q_ready[:, j * QK : j * QK + PLAIN]
        ql = dot(qn, ku_ref[:, j * PLAIN : (j + 1) * PLAIN], ((1,), (1,)))
        qs_ref[rows, :LAT] = (ql * LOG2E).astype(BF)
        qs_ref[rows, LAT:] = q_rope[:, j * QK + PLAIN : (j + 1) * QK]
    outs = []
    width = 2 * toks
    for half in range(GROUP // 2):
        cols = slice(half * width, (half + 1) * width)
        scores = dot(keys_ref[...], qs_ref[cols, :], ((1,), (1,)))
        top = jnp.max(scores, axis=0, keepdims=True)
        probs = jnp.exp2(scores - top)
        total = jnp.sum(probs, axis=0, keepdims=True)
        ctx = dot(klt_ref[...], probs.astype(BF), ((1,), (0,)))
        ctx = (ctx * (1.0 / total)).astype(BF)
        for j in range(2):
            h = half * 2 + j
            outs.append(
                dot(
                    vu_ref[:, h * PLAIN : (h + 1) * PLAIN],
                    ctx[:, j * toks : (j + 1) * toks],
                    ((0,), (0,)),
                ).astype(BF)
            )
    heads = jnp.concatenate(outs, axis=0)
    acc_ref[...] += dot(heads, wo_ref[...], ((0,), (0,)))

    @pl.when(g == pl.num_programs(0) - 1)
    def _():
        mixed = acc_ref[...]
        mixed_ref[...] = mixed
        ms = jnp.mean(mixed * mixed, axis=-1, keepdims=True)
        normed = (mixed * lax.rsqrt(ms + EPS) * gain_ref[...]).astype(BF)
        normed_ref[...] = normed
        n_rows = out_ref.shape[0]
        half_d = D // 2
        stacked = jnp.concatenate([normed[:, :half_d], normed[:, half_d:]], axis=0)
        row = lax.broadcasted_iota(jnp.int32, (n_rows, toks), 0)
        picks = []
        for h in range(2):
            m = (row == brow_ref[0:1, :] + 4 * h) | (row == brow_ref[1:2, :] + 4 * h)
            picks.append(jnp.where(m, 1.0, 0.0).astype(BF))
        pick = jnp.concatenate(picks, axis=1)
        out_ref[...] = dot(pick, stacked, ((1,), (0,))).astype(BF)


def expert_kernel(rows_ref, gate_ref, up_ref, down_ref, out_ref, x_ref, acc_ref):
    f = pl.program_id(0)
    n_src = rows_ref.shape[0]
    half_d = D // 2

    @pl.when(f == 0)
    def _():
        r = rows_ref[...].astype(F32).reshape(n_src // 2, 2, 8, half_d)
        a = r[:, 0].reshape(n_src * 4, half_d)
        b = r[:, 1].reshape(n_src * 4, half_d)
        sub = lax.broadcasted_iota(jnp.int32, a.shape, 0) % 8
        rolled = lambda v: pltpu.roll(v.reshape(n_src // 2, 8, half_d), 4, 1).reshape(v.shape)
        x_ref[:, :half_d] = jnp.where(sub < 4, a, rolled(b)).astype(BF)
        x_ref[:, half_d:] = jnp.where(sub < 4, rolled(a), b).astype(BF)

    x = x_ref[...]
    gate = dot(x, gate_ref[...], ((1,), (0,)))
    up = dot(x, up_ref[...], ((1,), (0,)))
    cut = jnp.minimum(gate, CLAMP)
    hidden = (cut * jax.nn.sigmoid(ALPHA * cut) * (jnp.clip(up, -CLAMP, CLAMP) + 1.0)).astype(BF)
    part = dot(hidden, down_ref[...], ((1,), (0,)))

    @pl.when(f == 0)
    def _():
        acc_ref[...] = part

    @pl.when(f > 0)
    def _():
        acc_ref[...] += part

    @pl.when(f == pl.num_programs(0) - 1)
    def _():
        lo = acc_ref[:, :half_d].reshape(n_src // 2, 8, half_d)
        hi = acc_ref[:, half_d:].reshape(n_src // 2, 8, half_d)
        sub = lax.broadcasted_iota(jnp.int32, lo.shape, 1)
        first = jnp.where(sub < 4, lo, pltpu.roll(hi, 4, 1))
        second = jnp.where(sub < 4, pltpu.roll(lo, 4, 1), hi)
        both = jnp.concatenate([first[:, None], second[:, None]], axis=1)
        out_ref[...] = both.reshape(n_src, 8, half_d).astype(BF)


def combine_kernel(rows_ref, bcol_ref, weight_ref, mixed_ref, out_ref):
    n_rows = rows_ref.shape[0]
    toks = mixed_ref.shape[0]
    half_d = D // 2
    lane = lax.broadcasted_iota(jnp.int32, (toks, n_rows), 1)
    for h in range(2):
        total = mixed_ref[:, h * half_d : (h + 1) * half_d]
        for k in range(TOPK):
            pick = jnp.where(lane == bcol_ref[:, k : k + 1] + 4 * h, 1.0, 0.0).astype(BF)
            total += weight_ref[:, k : k + 1] * dot(pick, rows_ref[...], ((1,), (0,)))
        out_ref[:, h * half_d : (h + 1) * half_d] = total.astype(BF)


def full(*shape):
    return pl.BlockSpec(shape, lambda *_: (0,) * len(shape))


def params(mb=60):
    return pltpu.CompilerParams(vmem_limit_bytes=mb * 1024 * 1024)


def local(
    queries, kv_latent, rope_key, latent_norm_gain, key_up_weight, value_up_weight, out_proj,
    residual, ffn_gain, routes, route_weights, expert_gate, expert_up, expert_down,
):
    toks = queries.shape[1]
    sp = lax.axis_size("sp")
    experts = sp * lax.axis_size("dp")
    keys_n = sp * toks
    sds = jax.ShapeDtypeStruct
    positions = lax.axis_index("sp") * toks + jnp.arange(toks, dtype=jnp.int32)
    kc, ks = lane_tables(positions, ROT)
    packed = pl.pallas_call(
        key_kernel, out_shape=sds((sp, toks, LAT + ROT), BF), compiler_params=params(), name="keys"
    )(kv_latent[0], rope_key[0], latent_norm_gain[None], kc, ks)
    keys = lax.all_to_all(packed, "sp", 0, 0, tiled=True).reshape(keys_n, LAT + ROT)

    qc, qs = lane_tables(positions, GROUP * QK)
    bcol, brow = pl.pallas_call(
        route_kernel,
        out_shape=(sds((toks, TOPK), jnp.int32), sds((TOPK, toks), jnp.int32)),
        compiler_params=params(),
        name="routes",
    )(routes[0], routes[0].T)

    steps = HEADS // GROUP
    mixed, normed, outgoing = pl.pallas_call(
        attend_kernel,
        grid=(steps,),
        in_specs=[
            pl.BlockSpec((toks, GROUP * QK), lambda g: (0, g)),
            full(toks, GROUP * QK),
            full(toks, GROUP * QK),
            full(keys_n, LAT + ROT),
            pl.BlockSpec((LAT, GROUP * PLAIN), lambda g: (0, g)),
            pl.BlockSpec((LAT, GROUP * PLAIN), lambda g: (0, g)),
            pl.BlockSpec((GROUP * PLAIN, D), lambda g: (g, 0)),
            full(toks, D),
            full(1, D),
            full(TOPK, toks),
        ],
        out_specs=(full(toks, D), full(toks, D), full(experts * 8, D // 2)),
        out_shape=(sds((toks, D), F32), sds((toks, D), BF), sds((experts * 8, D // 2), BF)),
        scratch_shapes=[
            pltpu.VMEM((LAT, keys_n), BF),
            pltpu.VMEM((GROUP * toks, LAT + ROT), BF),
            pltpu.VMEM((toks, D), F32),
        ],
        compiler_params=params(),
        name="attend",
    )(queries[0], qc, qs, keys, key_up_weight, value_up_weight, out_proj, residual[0],
      ffn_gain[None], brow)

    slot_rows = lax.all_to_all(
        outgoing.reshape(experts, 8, D // 2), ("sp", "dp"), 0, 0, tiled=True
    )
    f_steps = 4
    fb = FF // f_steps
    expert_out = pl.pallas_call(
        expert_kernel,
        grid=(f_steps,),
        in_specs=[
            full(experts, 8, D // 2),
            pl.BlockSpec((D, fb), lambda f: (0, f)),
            pl.BlockSpec((D, fb), lambda f: (0, f)),
            pl.BlockSpec((fb, D), lambda f: (f, 0)),
        ],
        out_specs=full(experts, 8, D // 2),
        out_shape=sds((experts, 8, D // 2), BF),
        scratch_shapes=[pltpu.VMEM((experts * CAP, D), BF), pltpu.VMEM((experts * CAP, D), F32)],
        compiler_params=params(),
        name="experts",
    )(slot_rows, expert_gate[0], expert_up[0], expert_down[0])
    returned = lax.all_to_all(expert_out, ("sp", "dp"), 0, 0, tiled=True)
    layer_out = pl.pallas_call(
        combine_kernel,
        out_shape=sds((toks, D), BF),
        compiler_params=params(),
        name="combine",
    )(returned.reshape(experts * 8, D // 2), bcol, route_weights[0], mixed)
    return normed[None], layer_out[None]


def solution(mesh):
    tok = P("dp", "sp", None)
    exp = P(("sp", "dp"), None, None)
    in_specs = (
        tok, tok, tok, P(), P(), P(), P(), tok, P(), tok, tok, exp, exp, exp,
    )
    return jax.shard_map(
        local, mesh=mesh, in_specs=in_specs, out_specs=(tok, tok), check_vma=False
    )
```

```python
import numpy as np
import jax
import jax.numpy as jnp
from jax import lax
from jax.experimental import pallas as pl
from jax.experimental.pallas import tpu as pltpu
from jax.sharding import PartitionSpec as P

D = 2048
HEADS = 32
PLAIN = 64
ROT = 32
QK = PLAIN + ROT
LAT = 256
TOPK = 2
GRID_W = 64
FF = 1024
CAP = 4
GROUP = 4
EPS = 1e-06
CLAMP = 7.0
ALPHA = 1.702
LOG2E = 1.4426950408889634
BF = jnp.bfloat16
F32 = jnp.float32


def prep_kernel(
    off_ref, lat_ref, rope_ref, gain_ref, freq_ref, out_ref, cos_ref, sin_ref
):
    toks = lat_ref.shape[0]
    p = off_ref[0] * toks + lax.broadcasted_iota(jnp.int32, (ROT, toks), 1)
    entry = lax.broadcasted_iota(jnp.int32, (ROT, toks), 0)
    place = jnp.where(entry < ROT // 2, p // GRID_W, p % GRID_W).astype(F32)
    angle = place * freq_ref[...]
    cosine = jnp.cos(angle)
    sine = jnp.where(entry % 2 == 0, -jnp.sin(angle), jnp.sin(angle))
    cos_ref[...] = cosine
    sin_ref[...] = sine
    lat = lat_ref[...].astype(F32)
    ms = jnp.mean(lat * lat, axis=-1, keepdims=True)
    latent = lat * lax.rsqrt(ms + EPS) * gain_ref[...]
    turned = turn(rope_ref[...].astype(F32).T, cosine, sine)
    both = jnp.concatenate([latent.T, turned], axis=0).astype(BF)
    for i in range(out_ref.shape[0]):
        out_ref[i] = both


def turn(x, cosine, sine):
    y = x.reshape(x.shape[0] // 8, 8, x.shape[1])
    even = lax.broadcasted_iota(jnp.int32, y.shape, 1) % 2 == 0
    swapped = jnp.where(even, pltpu.roll(y, 7, 1), pltpu.roll(y, 1, 1)).reshape(x.shape)
    return x * cosine + swapped * sine


def pair_frequencies():
    pair = np.arange(ROT) // 2 % (ROT // 4)
    return (10000.0 ** (-(2.0 * pair) / (ROT // 2))).astype(np.float32)[:, None]


def route_kernel(col_ref, row_ref, weight_ref, bcol_ref, brow_ref, wcol_ref):
    wcol_ref[...] = weight_ref[...]
    n = col_ref.shape[0]
    sub = lax.broadcasted_iota(jnp.int32, (n, n), 0)
    lane = lax.broadcasted_iota(jnp.int32, (n, n), 1)
    e_c = [col_ref[:, k : k + 1] for k in range(2)]
    e_r = [row_ref[k : k + 1, :] for k in range(2)]
    same00 = e_c[0] == e_r[0]
    same11 = e_c[1] == e_r[1]
    one = lambda m: jnp.where(m, 1.0, 0.0)
    r0 = jnp.sum(one(same00 & (lane < sub)), axis=1, keepdims=True)
    r1 = jnp.sum(one(same11 & (lane < sub)), axis=1, keepdims=True) + jnp.sum(
        one(e_c[1] == e_r[0]), axis=1, keepdims=True
    )
    bcol_ref[:, 0:1] = e_c[0] * 8 + r0.astype(jnp.int32)
    bcol_ref[:, 1:2] = e_c[1] * 8 + r1.astype(jnp.int32)
    s0 = jnp.sum(one(same00 & (sub < lane)), axis=0, keepdims=True)
    s1 = jnp.sum(one(same11 & (sub < lane)), axis=0, keepdims=True) + jnp.sum(
        one(e_c[0] == e_r[1]), axis=0, keepdims=True
    )
    brow_ref[0:1, :] = e_r[0] * 8 + s0.astype(jnp.int32)
    brow_ref[1:2, :] = e_r[1] * 8 + s1.astype(jnp.int32)


def dot(a, b, dims):
    return lax.dot_general(a, b, (dims, ((), ())), preferred_element_type=F32)


def attend_kernel(
    q_ref, cos_ref, sin_ref, kt_ref, ku_ref, vup_ref, vuc_ref, wo_ref, res_ref, gain_ref, brow_ref,
    mixed_ref, normed_ref, out_ref,
    keys_ref, klt_ref, bd_ref, qa_ref, qb_ref, sa_ref, sb_ref, pa_ref, pb_ref, mb_ref, heads_ref, acc_ref,
):
    g = pl.program_id(0)
    last = pl.num_programs(0) - 1
    toks = q_ref.shape[0]
    width = 2 * toks
    n_keys = keys_ref.shape[0]
    chunk = 256
    chunks = n_keys // chunk

    @pl.when(g == 0)
    def _():
        for i in range(kt_ref.shape[0]):
            rows = slice(i * toks, (i + 1) * toks)
            klt_ref[:, rows] = kt_ref[i, :LAT, :]
            keys_ref[rows, :] = kt_ref[i].T
        bd_ref[...] = jnp.zeros_like(bd_ref)

    def pieces(x):
        return x.reshape(x.shape[0] // 8, 8, x.shape[1])

    def score_chunk(q, s_ref, i, top):
        rows = slice(i * chunk, (i + 1) * chunk)
        s = dot(keys_ref[rows, :], q, ((1,), (0,)))
        s_ref[rows, :] = s
        part = jnp.max(pieces(s), axis=0)
        return part if top is None else jnp.maximum(top, part)

    def prob_chunk(s_ref, p_ref, i, top, total):
        rows = slice(i * chunk, (i + 1) * chunk)
        p = jnp.exp2(s_ref[rows, :] - top)
        p_ref[rows, :] = p.astype(BF)
        part = jnp.sum(pieces(p), axis=0)
        return part if total is None else total + part

    def heads_of(p_ref, total, vt):
        ctx = dot(klt_ref[...], p_ref[...], ((1,), (0,)))
        inv = 1.0 / jnp.sum(total, axis=0, keepdims=True)
        both = dot(vt, (ctx * inv).astype(BF), ((1,), (0,)))
        return jnp.concatenate([both[:PLAIN, :toks], both[PLAIN:, toks:]], axis=0).astype(BF)

    def project():
        acc_ref[...] += dot(heads_ref[...], wo_ref[...], ((0,), (0,)))

    @pl.when(g < last)
    def _():
        qt = q_ref[...].astype(F32).T * (QK ** -0.5)
        for j in range(GROUP):
            bd_ref[j * PLAIN : (j + 1) * PLAIN, j * toks : (j + 1) * toks] = qt[
                j * QK : j * QK + PLAIN
            ].astype(BF)
        ql = (dot(ku_ref[...], bd_ref[...], ((1,), (0,))) * LOG2E).astype(BF)
        for half, dst in enumerate((qa_ref, qb_ref)):
            dst[:LAT, :] = ql[:, half * width : (half + 1) * width]
            for j in range(2):
                r = (half * 2 + j) * QK + PLAIN
                turned = turn(qt[r : r + ROT], cos_ref[...], sin_ref[...])
                dst[LAT:, j * toks : (j + 1) * toks] = (turned * LOG2E).astype(BF)

        qa = qa_ref[...]
        top, total = None, None
        prev = mb_ref[...]
        for i in range(chunks):
            top = score_chunk(qa, sa_ref, i, top)
            total = prob_chunk(sb_ref, pb_ref, i, prev, total)
        top_a = jnp.max(top, axis=0, keepdims=True)
        heads_ref[width // 2 :, :] = heads_of(pb_ref, total, vup_ref[2 * PLAIN :, :])
        project()
        qb = qb_ref[...]
        top, total = None, None
        for i in range(chunks):
            top = score_chunk(qb, sb_ref, i, top)
            total = prob_chunk(sa_ref, pa_ref, i, top_a, total)
        mb_ref[...] = jnp.max(top, axis=0, keepdims=True)
        heads_ref[: width // 2, :] = heads_of(pa_ref, total, vuc_ref[: 2 * PLAIN, :])

    @pl.when(g == 0)
    def _():
        acc_ref[...] = res_ref[...].astype(F32)

    @pl.when(g == last)
    def _():
        total = None
        prev = mb_ref[...]
        for i in range(chunks):
            total = prob_chunk(sb_ref, pb_ref, i, prev, total)
        heads_ref[width // 2 :, :] = heads_of(pb_ref, total, vup_ref[2 * PLAIN :, :])
        project()
        mixed = acc_ref[...]
        mixed_ref[...] = mixed
        ms = jnp.mean(mixed * mixed, axis=-1, keepdims=True)
        normed = (mixed * lax.rsqrt(ms + EPS) * gain_ref[...]).astype(BF)
        normed_ref[...] = normed
        n_rows = out_ref.shape[0]
        half_d = D // 2
        stacked = jnp.concatenate([normed[:, :half_d], normed[:, half_d:]], axis=0)
        row = lax.broadcasted_iota(jnp.int32, (n_rows, toks), 0)
        picks = []
        for h in range(2):
            m = (row == brow_ref[0:1, :] + 4 * h) | (row == brow_ref[1:2, :] + 4 * h)
            picks.append(jnp.where(m, 1.0, 0.0).astype(BF))
        pick = jnp.concatenate(picks, axis=1)
        out_ref[...] = dot(pick, stacked, ((1,), (0,))).astype(BF)


def expert_kernel(rows_ref, gate_ref, up_ref, lo_ref, hi_ref, out_ref, x_ref, hidden_ref):
    f = pl.program_id(0)
    n_src = rows_ref.shape[0]
    half_d = D // 2
    fb = gate_ref.shape[1]
    f_steps = FF // fb

    @pl.when(f == 0)
    def _():
        r = rows_ref[...].astype(F32).reshape(n_src // 2, 2, 8, half_d)
        a, b = r[:, 0], r[:, 1]
        low = lax.broadcasted_iota(jnp.int32, a.shape, 1) < 4
        first = jnp.where(low, a, pltpu.roll(b, 4, 1))
        second = jnp.where(low, pltpu.roll(a, 4, 1), b)
        x_ref[:, :half_d] = first.reshape(n_src * 4, half_d).astype(BF)
        x_ref[:, half_d:] = second.reshape(n_src * 4, half_d).astype(BF)

    @pl.when(f < f_steps)
    def _():
        x = x_ref[...]
        gate = dot(x, gate_ref[...], ((1,), (0,)))
        up = dot(x, up_ref[...], ((1,), (0,)))
        cut = jnp.minimum(gate, CLAMP)
        act = cut * jax.nn.sigmoid(ALPHA * cut) * (jnp.clip(up, -CLAMP, CLAMP) + 1.0)
        hidden_ref[f] = act.astype(BF)

    @pl.when(f >= f_steps)
    def _():
        hidden = jnp.concatenate([hidden_ref[i] for i in range(f_steps)], axis=1)
        lanes = lo_ref.shape[1]
        lo = dot(hidden, lo_ref[...], ((1,), (0,))).reshape(n_src // 2, 8, lanes)
        hi = dot(hidden, hi_ref[...], ((1,), (0,))).reshape(n_src // 2, 8, lanes)
        low = lax.broadcasted_iota(jnp.int32, lo.shape, 1) < 4
        first = jnp.where(low, lo, pltpu.roll(hi, 4, 1))
        second = jnp.where(low, pltpu.roll(lo, 4, 1), hi)
        both = jnp.concatenate([first[:, None], second[:, None]], axis=1)
        out_ref[...] = both.reshape(n_src, 8, lanes).astype(BF)


def combine_kernel(rows_ref, bcol_ref, weight_ref, mixed_ref, out_ref, pick_ref):
    n = pl.program_id(0)
    n_rows = rows_ref.shape[0]
    toks = mixed_ref.shape[0]
    per = pl.num_programs(0) // 2

    @pl.when(n % per == 0)
    def _():
        lane = lax.broadcasted_iota(jnp.int32, (toks, n_rows), 1)
        shift = 4 * (n // per)
        for k in range(TOPK):
            pick = jnp.where(lane == bcol_ref[:, k : k + 1] + shift, 1.0, 0.0).astype(BF)
            pick_ref[k * toks : (k + 1) * toks, :] = pick

    got = dot(pick_ref[...], rows_ref[...], ((1,), (0,)))
    total = mixed_ref[...]
    for k in range(TOPK):
        total += weight_ref[:, k : k + 1] * got[k * toks : (k + 1) * toks]
    out_ref[...] = total.astype(BF)


def full(*shape):
    return pl.BlockSpec(shape, lambda *_: (0,) * len(shape))


def params(mb=60):
    return pltpu.CompilerParams(vmem_limit_bytes=mb * 1024 * 1024)


def attend(q, ct, st, keys, ku, vut, wo, res, gain, brow, experts):
    sds = jax.ShapeDtypeStruct
    toks = q.shape[0]
    keys_n = keys.shape[0] * toks
    steps = HEADS // GROUP
    now = lambda g: jnp.minimum(g, steps - 1)
    before = lambda g: jnp.maximum(g - 1, 0)
    return pl.pallas_call(
        attend_kernel,
        grid=(steps + 1,),
        in_specs=[
            pl.BlockSpec((toks, GROUP * QK), lambda g: (0, now(g))),
            full(ROT, toks),
            full(ROT, toks),
            full(*keys.shape),
            pl.BlockSpec((LAT, GROUP * PLAIN), lambda g: (0, now(g))),
            pl.BlockSpec((GROUP * PLAIN, LAT), lambda g: (before(g), 0)),
            pl.BlockSpec((GROUP * PLAIN, LAT), lambda g: (now(g), 0)),
            pl.BlockSpec((GROUP * PLAIN, D), lambda g: (before(g), 0)),
            full(toks, D),
            full(1, D),
            full(TOPK, toks),
        ],
        out_specs=(full(toks, D), full(toks, D), full(experts * 8, D // 2)),
        out_shape=(sds((toks, D), F32), sds((toks, D), BF), sds((experts * 8, D // 2), BF)),
        scratch_shapes=[
            pltpu.VMEM((keys_n, LAT + ROT), BF),
            pltpu.VMEM((LAT, keys_n), BF),
            pltpu.VMEM((GROUP * PLAIN, GROUP * toks), BF),
            pltpu.VMEM((LAT + ROT, 2 * toks), BF),
            pltpu.VMEM((LAT + ROT, 2 * toks), BF),
            pltpu.VMEM((keys_n, 2 * toks), F32),
            pltpu.VMEM((keys_n, 2 * toks), F32),
            pltpu.VMEM((keys_n, 2 * toks), BF),
            pltpu.VMEM((keys_n, 2 * toks), BF),
            pltpu.VMEM((1, 2 * toks), F32),
            pltpu.VMEM((GROUP * PLAIN, toks), BF),
            pltpu.VMEM((toks, D), F32),
        ],
        compiler_params=params(),
        name="attend",
    )(q, ct, st, keys, ku, vut, vut, wo, res, gain, brow)


def local(
    queries, kv_latent, rope_key, latent_norm_gain, key_up_weight, value_up_weight, out_proj,
    residual, ffn_gain, routes, route_weights, expert_gate, expert_up, expert_down,
):
    toks = queries.shape[1]
    sp = lax.axis_size("sp")
    experts = sp * lax.axis_size("dp")
    sds = jax.ShapeDtypeStruct
    offset = lax.axis_index("sp").astype(jnp.int32)[None]
    packed, ct, st = pl.pallas_call(
        prep_kernel,
        in_specs=[pl.BlockSpec(memory_space=pltpu.SMEM)] + [pl.BlockSpec()] * 4,
        out_shape=(sds((sp, LAT + ROT, toks), BF), sds((ROT, toks), F32), sds((ROT, toks), F32)),
        compiler_params=params(),
        name="prep",
    )(offset, kv_latent[0], rope_key[0], latent_norm_gain[None], pair_frequencies())
    keys = lax.all_to_all(packed, "sp", 0, 0, tiled=True)
    bcol, brow, wcol = pl.pallas_call(
        route_kernel,
        out_shape=(
            sds((toks, TOPK), jnp.int32), sds((TOPK, toks), jnp.int32), sds((toks, TOPK), F32)
        ),
        compiler_params=params(),
        name="routes",
    )(routes[0], routes[0].T, route_weights[0])

    mixed, normed, outgoing = attend(
        queries[0], ct, st, keys, key_up_weight, value_up_weight.T, out_proj, residual[0],
        ffn_gain[None], brow, experts,
    )

    slot_rows = lax.all_to_all(
        outgoing.reshape(experts, 8, D // 2), ("sp", "dp"), 0, 0, tiled=True
    )
    f_steps, o_steps = 4, 2
    fb, lanes = FF // f_steps, D // 2 // o_steps
    low = lambda f: jnp.minimum(f, f_steps - 1)
    out_at = lambda f: jnp.maximum(f - f_steps, 0)
    expert_out = pl.pallas_call(
        expert_kernel,
        grid=(f_steps + o_steps,),
        in_specs=[
            full(experts, 8, D // 2),
            pl.BlockSpec((D, fb), lambda f: (0, low(f))),
            pl.BlockSpec((D, fb), lambda f: (0, low(f))),
            pl.BlockSpec((FF, lanes), lambda f: (0, out_at(f))),
            pl.BlockSpec((FF, lanes), lambda f: (0, out_at(f) + o_steps)),
        ],
        out_specs=pl.BlockSpec((experts, 8, lanes), lambda f: (0, 0, out_at(f))),
        out_shape=sds((experts, 8, D // 2), BF),
        scratch_shapes=[
            pltpu.VMEM((experts * CAP, D), BF), pltpu.VMEM((f_steps, experts * CAP, fb), BF)
        ],
        compiler_params=params(),
        name="experts",
    )(slot_rows, expert_gate[0], expert_up[0], expert_down[0], expert_down[0])
    returned = lax.all_to_all(expert_out, ("sp", "dp"), 0, 0, tiled=True)
    per = 2
    layer_out = pl.pallas_call(
        combine_kernel,
        grid=(2 * per,),
        in_specs=[
            pl.BlockSpec((experts * 8, D // 2 // per), lambda n: (0, n % per)),
            full(toks, TOPK),
            full(toks, TOPK),
            pl.BlockSpec((toks, D // 2 // per), lambda n: (0, n)),
        ],
        out_specs=pl.BlockSpec((toks, D // 2 // per), lambda n: (0, n)),
        out_shape=sds((toks, D), BF),
        scratch_shapes=[pltpu.VMEM((TOPK * toks, experts * 8), BF)],
        compiler_params=params(),
        name="combine",
    )(returned.reshape(experts * 8, D // 2), bcol, wcol, mixed)
    return normed[None], layer_out[None]


def solution(mesh):
    tok = P("dp", "sp", None)
    exp = P(("sp", "dp"), None, None)
    in_specs = (
        tok, tok, tok, P(), P(), P(), P(), tok, P(), tok, tok, exp, exp, exp,
    )
    return jax.shard_map(
        local, mesh=mesh, in_specs=in_specs, out_specs=(tok, tok), check_vma=False
    )
```

```python
import numpy as np
import jax
import jax.numpy as jnp
from jax import lax
from jax.experimental import pallas as pl
from jax.experimental.pallas import tpu as pltpu
from jax.sharding import PartitionSpec as P

D = 2048
HEADS = 32
PLAIN = 64
ROT = 32
QK = PLAIN + ROT
LAT = 256
TOPK = 2
GRID_W = 64
FF = 1024
CAP = 4
GROUP = 4
CHUNK = 256
EPS = 1e-06
CLAMP = 7.0
ALPHA = 1.702
LOG2E = 1.4426950408889634
BF = jnp.bfloat16
F32 = jnp.float32


def prep_kernel(
    off_ref, lat_ref, rope_ref, gain_ref, freq_ref, out_ref, cos_ref, sin_ref
):
    toks = lat_ref.shape[0]
    p = off_ref[0] * toks + lax.broadcasted_iota(jnp.int32, (ROT, toks), 1)
    entry = lax.broadcasted_iota(jnp.int32, (ROT, toks), 0)
    place = jnp.where(entry < ROT // 2, p // GRID_W, p % GRID_W).astype(F32)
    angle = place * freq_ref[...]
    cosine = jnp.cos(angle)
    sine = jnp.where(entry % 2 == 0, -jnp.sin(angle), jnp.sin(angle))
    cos_ref[...] = cosine
    sin_ref[...] = sine
    lat = lat_ref[...].astype(F32)
    ms = jnp.mean(lat * lat, axis=-1, keepdims=True)
    latent = lat * lax.rsqrt(ms + EPS) * gain_ref[...]
    turned = turn(rope_ref[...].astype(F32), cosine, sine)
    both = jnp.concatenate([latent.T, turned], axis=0).astype(BF)
    for i in range(out_ref.shape[0]):
        out_ref[i] = both


def turn(x, cosine, sine):
    y = x.reshape(x.shape[0] // 8, 8, x.shape[1])
    even = lax.broadcasted_iota(jnp.int32, y.shape, 1) % 2 == 0
    swapped = jnp.where(even, pltpu.roll(y, 7, 1), pltpu.roll(y, 1, 1)).reshape(x.shape)
    return x * cosine + swapped * sine


def pair_frequencies():
    pair = np.arange(ROT) // 2 % (ROT // 4)
    return (10000.0 ** (-(2.0 * pair) / (ROT // 2))).astype(np.float32)[:, None]


def route_kernel(col_ref, row_ref, weight_ref, bcol_ref, brow_ref, wcol_ref):
    wcol_ref[...] = weight_ref[...]
    n = col_ref.shape[0]
    sub = lax.broadcasted_iota(jnp.int32, (n, n), 0)
    lane = lax.broadcasted_iota(jnp.int32, (n, n), 1)
    e_c = [col_ref[:, k : k + 1] for k in range(2)]
    e_r = [row_ref[k : k + 1, :] for k in range(2)]
    same00 = e_c[0] == e_r[0]
    same11 = e_c[1] == e_r[1]
    one = lambda m: jnp.where(m, 1.0, 0.0)
    r0 = jnp.sum(one(same00 & (lane < sub)), axis=1, keepdims=True)
    r1 = jnp.sum(one(same11 & (lane < sub)), axis=1, keepdims=True) + jnp.sum(
        one(e_c[1] == e_r[0]), axis=1, keepdims=True
    )
    bcol_ref[:, 0:1] = e_c[0] * 8 + r0.astype(jnp.int32)
    bcol_ref[:, 1:2] = e_c[1] * 8 + r1.astype(jnp.int32)
    s0 = jnp.sum(one(same00 & (sub < lane)), axis=0, keepdims=True)
    s1 = jnp.sum(one(same11 & (sub < lane)), axis=0, keepdims=True) + jnp.sum(
        one(e_c[0] == e_r[1]), axis=0, keepdims=True
    )
    brow_ref[0:1, :] = e_r[0] * 8 + s0.astype(jnp.int32)
    brow_ref[1:2, :] = e_r[1] * 8 + s1.astype(jnp.int32)


def dot(a, b, dims):
    return lax.dot_general(a, b, (dims, ((), ())), preferred_element_type=F32)


def query_kernel(q_ref, cos_ref, sin_ref, ku_ref, out_ref, bd_ref):
    toks = q_ref.shape[0]

    @pl.when(pl.program_id(0) == 0)
    def _():
        bd_ref[...] = jnp.zeros_like(bd_ref)

    qt = q_ref[...].astype(F32).T * (QK ** -0.5)
    for j in range(GROUP):
        bd_ref[j * PLAIN : (j + 1) * PLAIN, j * toks : (j + 1) * toks] = qt[
            j * QK : j * QK + PLAIN
        ].astype(BF)
    out_ref[0, :LAT, :] = (dot(ku_ref[...], bd_ref[...], ((1,), (0,))) * LOG2E).astype(BF)
    for j in range(GROUP):
        r = j * QK + PLAIN
        turned = turn(qt[r : r + ROT], cos_ref[...], sin_ref[...])
        out_ref[0, LAT:, j * toks : (j + 1) * toks] = (turned * LOG2E).astype(BF)


def attend_kernel(
    kt_ref, q0_ref, qb_ref, qa_ref, vb_ref, va_ref, vl_ref, wb_ref, wa_ref, wl_ref, res_ref,
    gain_ref, brow_ref, mixed_ref, normed_ref, out_ref,
    keys_ref, klt_ref, sa_ref, sb_ref, pa_ref, pb_ref, ta_ref, lb_ref, acc_ref,
):
    g = pl.program_id(0)
    last = pl.num_programs(0) - 1
    toks = res_ref.shape[0]
    n_keys = keys_ref.shape[0]
    chunk = CHUNK
    chunks = n_keys // chunk

    def pieces(x):
        return x.reshape(x.shape[0] // 8, 8, x.shape[1])

    def score_chunk(q, s_ref, i, top):
        rows = slice(i * chunk, (i + 1) * chunk)
        s = dot(keys_ref[rows, :], q, ((1,), (0,)))
        s_ref[rows, :] = s
        part = jnp.max(pieces(s), axis=0)
        return part if top is None else jnp.maximum(top, part)

    def prob_chunk(s_ref, p_ref, i, top, total):
        rows = slice(i * chunk, (i + 1) * chunk)
        p = jnp.exp2(s_ref[rows, :] - top)
        p_ref[rows, :] = p.astype(BF)
        part = jnp.sum(pieces(p), axis=0)
        return part if total is None else total + part

    def context(p_ref, total):
        ctx = dot(klt_ref[...], p_ref[...], ((1,), (0,)))
        return (ctx * (1.0 / jnp.sum(total, axis=0, keepdims=True))).astype(BF)

    def heads_of(ctx, vt):
        full_out = dot(vt, ctx, ((1,), (0,)))
        own = [
            full_out[j * PLAIN : (j + 1) * PLAIN, j * toks : (j + 1) * toks] for j in range(GROUP)
        ]
        return jnp.concatenate(own, axis=0).astype(BF)

    def project(heads, w_ref):
        acc_ref[...] += dot(heads, w_ref[...], ((0,), (0,)))

    def stage(q_ref, s_new, s_old, p_new, p_old, top_old, total_old, v_ref, w_ref):
        top, total, ctx, heads = None, None, None, None
        for i in range(chunks):
            if q_ref is not None:
                top = score_chunk(q_ref[0], s_new, i, top)
            total = prob_chunk(s_old, p_new, i, top_old, total)
            if i == chunks // 8:
                ctx = context(p_old, total_old)
            if i == chunks // 2:
                heads = heads_of(ctx, v_ref[...])
            if i == chunks * 3 // 4:
                project(heads, w_ref)
        if q_ref is not None:
            top = jnp.max(top, axis=0, keepdims=True)
        return top, total

    @pl.when(g == 0)
    def _():
        for i in range(kt_ref.shape[0]):
            rows = slice(i * toks, (i + 1) * toks)
            klt_ref[:, rows] = kt_ref[i, :LAT, :]
            keys_ref[rows, :] = kt_ref[i].T
        top = None
        for i in range(chunks):
            top = score_chunk(q0_ref[0], sa_ref, i, top)
        ta_ref[...] = jnp.max(top, axis=0, keepdims=True)

    top_b, total_a = stage(
        qb_ref, sb_ref, sa_ref, pa_ref, pb_ref, ta_ref[...], lb_ref[...], vb_ref, wb_ref
    )

    @pl.when(g == 0)
    def _():
        acc_ref[...] = res_ref[...].astype(F32)

    @pl.when(g < last)
    def _():
        top_a, total_b = stage(
            qa_ref, sa_ref, sb_ref, pb_ref, pa_ref, top_b, total_a, va_ref, wa_ref
        )
        ta_ref[...] = top_a
        lb_ref[...] = total_b

    @pl.when(g == last)
    def _():
        _, total_b = stage(
            None, sa_ref, sb_ref, pb_ref, pa_ref, top_b, total_a, va_ref, wa_ref
        )
        project(heads_of(context(pb_ref, total_b), vl_ref[...]), wl_ref)
        mixed = acc_ref[...]
        mixed_ref[...] = mixed
        ms = jnp.mean(mixed * mixed, axis=-1, keepdims=True)
        normed = (mixed * lax.rsqrt(ms + EPS) * gain_ref[...]).astype(BF)
        normed_ref[...] = normed
        n_rows = out_ref.shape[0]
        half_d = D // 2
        stacked = jnp.concatenate([normed[:, :half_d], normed[:, half_d:]], axis=0)
        row = lax.broadcasted_iota(jnp.int32, (n_rows, toks), 0)
        picks = []
        for h in range(2):
            m = (row == brow_ref[0:1, :] + 4 * h) | (row == brow_ref[1:2, :] + 4 * h)
            picks.append(jnp.where(m, 1.0, 0.0).astype(BF))
        pick = jnp.concatenate(picks, axis=1)
        out_ref[...] = dot(pick, stacked, ((1,), (0,))).astype(BF)


def expert_kernel(
    rows_ref, gate_ref, up_hbm, down_hbm, out_ref, x_ref, hidden_ref, up_ref, down_ref, sem_ref
):
    f = pl.program_id(0)
    copy_up = pltpu.make_async_copy(up_hbm, up_ref, sem_ref.at[0])
    copy_down = pltpu.make_async_copy(down_hbm, down_ref, sem_ref.at[1])
    n_src = rows_ref.shape[0]
    half_d = D // 2
    f_steps, _, fb = hidden_ref.shape
    lanes = out_ref.shape[2]

    @pl.when(f == 0)
    def _():
        copy_up.start()
        copy_down.start()
        r = rows_ref[...].astype(F32).reshape(n_src // 2, 2, 8, half_d)
        a, b = r[:, 0], r[:, 1]
        low = lax.broadcasted_iota(jnp.int32, a.shape, 1) < 4
        first = jnp.where(low, a, pltpu.roll(b, 4, 1))
        second = jnp.where(low, pltpu.roll(a, 4, 1), b)
        x_ref[:, :half_d] = first.reshape(n_src * 4, half_d).astype(BF)
        x_ref[:, half_d:] = second.reshape(n_src * 4, half_d).astype(BF)

    @pl.when(f == 0)
    def _():
        copy_up.wait()

    @pl.when(f == f_steps)
    def _():
        copy_down.wait()

    @pl.when(f < f_steps)
    def _():
        x = x_ref[...]
        cols = pl.ds(pl.multiple_of(f * fb, fb), fb)
        gate = dot(x, gate_ref[:, cols], ((1,), (0,)))
        up = dot(x, up_ref[:, cols], ((1,), (0,)))
        cut = jnp.minimum(gate, CLAMP)
        act = cut * jax.nn.sigmoid(ALPHA * cut) * (jnp.clip(up, -CLAMP, CLAMP) + 1.0)
        hidden_ref[f] = act.astype(BF)

    @pl.when(f >= f_steps)
    def _():
        hidden = jnp.concatenate([hidden_ref[i] for i in range(f_steps)], axis=1)
        at = pl.multiple_of((f - f_steps) * lanes, lanes)
        lo = dot(hidden, down_ref[:, pl.ds(at, lanes)], ((1,), (0,)))
        hi = dot(hidden, down_ref[:, pl.ds(at + half_d, lanes)], ((1,), (0,)))
        lo = lo.reshape(n_src // 2, 8, lanes)
        hi = hi.reshape(n_src // 2, 8, lanes)
        low = lax.broadcasted_iota(jnp.int32, lo.shape, 1) < 4
        first = jnp.where(low, lo, pltpu.roll(hi, 4, 1))
        second = jnp.where(low, pltpu.roll(lo, 4, 1), hi)
        both = jnp.concatenate([first[:, None], second[:, None]], axis=1)
        out_ref[...] = both.reshape(n_src, 8, lanes).astype(BF)


def combine_kernel(rows_ref, bcol_ref, weight_ref, mixed_ref, out_ref, pick_ref):
    n = pl.program_id(0)
    n_rows = rows_ref.shape[0]
    toks = mixed_ref.shape[0]
    per = pl.num_programs(0) // 2

    @pl.when(n % per == 0)
    def _():
        lane = lax.broadcasted_iota(jnp.int32, (toks, n_rows), 1)
        shift = 4 * (n // per)
        for k in range(TOPK):
            pick = jnp.where(lane == bcol_ref[:, k : k + 1] + shift, 1.0, 0.0).astype(BF)
            pick_ref[k * toks : (k + 1) * toks, :] = pick

    lanes = mixed_ref.shape[1]
    cols = pl.ds(pl.multiple_of(n % per * lanes, lanes), lanes)
    got = dot(pick_ref[...], rows_ref[:, cols], ((1,), (0,)))
    total = mixed_ref[...]
    for k in range(TOPK):
        total += weight_ref[:, k : k + 1] * got[k * toks : (k + 1) * toks]
    out_ref[...] = total.astype(BF)


def in_vmem(x):
    return pltpu.with_memory_space_constraint(x, pltpu.VMEM)


def in_hbm(x):
    return pltpu.with_memory_space_constraint(x, pltpu.HBM)


def whole():
    return pl.BlockSpec(memory_space=pltpu.VMEM)


def full(*shape):
    return pl.BlockSpec(shape, lambda *_: (0,) * len(shape))


def params(mb=60):
    return pltpu.CompilerParams(vmem_limit_bytes=mb * 1024 * 1024)


def ready_queries(q, ct, st, ku):
    toks = q.shape[0]
    return pl.pallas_call(
        query_kernel,
        grid=(HEADS // GROUP,),
        in_specs=[
            pl.BlockSpec((toks, GROUP * QK), lambda g: (0, g)),
            full(ROT, toks),
            full(ROT, toks),
            pl.BlockSpec((LAT, GROUP * PLAIN), lambda g: (0, g)),
        ],
        out_specs=pl.BlockSpec((1, LAT + ROT, GROUP * toks), lambda g: (g, 0, 0)),
        out_shape=jax.ShapeDtypeStruct((HEADS // GROUP, LAT + ROT, GROUP * toks), BF),
        scratch_shapes=[pltpu.VMEM((GROUP * PLAIN, GROUP * toks), BF)],
        compiler_params=params(24),
        name="queries",
    )(q, ct, st, ku)


def attend(qs, keys, vut, wo, res, gain, brow, experts):
    sds = jax.ShapeDtypeStruct
    toks = res.shape[0]
    keys_n = keys.shape[0] * toks
    groups = HEADS // GROUP
    before = lambda g: jnp.maximum(2 * g - 1, 0)
    q_at = lambda f: pl.BlockSpec((1, LAT + ROT, GROUP * toks), lambda g: (f(g), 0, 0))
    v_at = lambda f: pl.BlockSpec((GROUP * PLAIN, LAT), lambda g: (f(g), 0))
    w_at = lambda f: pl.BlockSpec((GROUP * PLAIN, D), lambda g: (f(g), 0))
    return pl.pallas_call(
        attend_kernel,
        grid=(groups // 2,),
        in_specs=[
            whole(),
            q_at(lambda g: 0),
            q_at(lambda g: 2 * g + 1),
            q_at(lambda g: jnp.minimum(2 * g + 2, groups - 1)),
            v_at(before),
            v_at(lambda g: 2 * g),
            v_at(lambda g: groups - 1),
            w_at(before),
            w_at(lambda g: 2 * g),
            w_at(lambda g: groups - 1),
            full(toks, D),
            full(1, D),
            full(TOPK, toks),
        ],
        out_specs=(full(toks, D), full(toks, D), full(experts * 8, D // 2)),
        out_shape=(sds((toks, D), F32), sds((toks, D), BF), sds((experts * 8, D // 2), BF)),
        scratch_shapes=[
            pltpu.VMEM((keys_n, LAT + ROT), BF),
            pltpu.VMEM((LAT, keys_n), BF),
            pltpu.VMEM((keys_n, GROUP * toks), F32),
            pltpu.VMEM((keys_n, GROUP * toks), F32),
            pltpu.VMEM((keys_n, GROUP * toks), BF),
            pltpu.VMEM((keys_n, GROUP * toks), BF),
            pltpu.VMEM((1, GROUP * toks), F32),
            pltpu.VMEM((8, GROUP * toks), F32),
            pltpu.VMEM((toks, D), F32),
        ],
        compiler_params=params(44),
        name="attend",
    )(keys, qs, qs, qs, vut, vut, vut, wo, wo, wo, res, gain, brow)


def local(
    queries, kv_latent, rope_key, latent_norm_gain, key_up_weight, value_up_weight, out_proj,
    residual, ffn_gain, routes, route_weights, expert_gate, expert_up, expert_down,
):
    toks = queries.shape[1]
    sp = lax.axis_size("sp")
    experts = sp * lax.axis_size("dp")
    sds = jax.ShapeDtypeStruct
    offset = lax.axis_index("sp").astype(jnp.int32)[None]
    packed, ct, st = pl.pallas_call(
        prep_kernel,
        in_specs=[pl.BlockSpec(memory_space=pltpu.SMEM)] + [pl.BlockSpec()] * 4,
        out_shape=(sds((sp, LAT + ROT, toks), BF), sds((ROT, toks), F32), sds((ROT, toks), F32)),
        compiler_params=params(),
        name="prep",
    )(offset, kv_latent[0], rope_key[0].T, latent_norm_gain[None], pair_frequencies())
    keys = in_vmem(lax.all_to_all(packed, "sp", 0, 0, tiled=True))
    bcol, brow, wcol = pl.pallas_call(
        route_kernel,
        out_shape=(
            sds((toks, TOPK), jnp.int32), sds((TOPK, toks), jnp.int32), sds((toks, TOPK), F32)
        ),
        compiler_params=params(),
        name="routes",
    )(routes[0], routes[0].T, route_weights[0])

    mixed, normed, outgoing = attend(
        ready_queries(queries[0], ct, st, key_up_weight), keys, value_up_weight.T, out_proj,
        in_hbm(residual[0]), ffn_gain[None], brow, experts,
    )

    slot_rows = lax.all_to_all(
        outgoing.reshape(experts, 8, D // 2), ("sp", "dp"), 0, 0, tiled=True
    )
    f_steps, o_steps = 4, 2
    fb, lanes = FF // f_steps, D // 2 // o_steps
    out_at = lambda f: jnp.maximum(f - f_steps, 0)
    expert_out = pl.pallas_call(
        expert_kernel,
        grid=(f_steps + o_steps,),
        in_specs=[whole()] * 2 + [pl.BlockSpec(memory_space=pl.ANY)] * 2,
        out_specs=pl.BlockSpec((experts, 8, lanes), lambda f: (0, 0, out_at(f))),
        out_shape=sds((experts, 8, D // 2), BF),
        scratch_shapes=[
            pltpu.VMEM((experts * CAP, D), BF),
            pltpu.VMEM((f_steps, experts * CAP, fb), BF),
            pltpu.VMEM((D, FF), BF),
            pltpu.VMEM((FF, D), BF),
            pltpu.SemaphoreType.DMA((2,)),
        ],
        compiler_params=params(40),
        name="experts",
    )(
        in_vmem(slot_rows),
        in_vmem(expert_gate[0]),
        expert_up[0],
        expert_down[0],
    )
    returned = lax.all_to_all(expert_out, ("sp", "dp"), 0, 0, tiled=True)
    per = 2
    layer_out = pl.pallas_call(
        combine_kernel,
        grid=(2 * per,),
        in_specs=[
            whole(),
            full(toks, TOPK),
            full(toks, TOPK),
            pl.BlockSpec((toks, D // 2 // per), lambda n: (0, n)),
        ],
        out_specs=pl.BlockSpec((toks, D // 2 // per), lambda n: (0, n)),
        out_shape=sds((toks, D), BF),
        scratch_shapes=[pltpu.VMEM((TOPK * toks, experts * 8), BF)],
        compiler_params=params(40),
        name="combine",
    )(in_vmem(returned.reshape(experts * 8, D // 2)), bcol, wcol, mixed)
    return normed[None], layer_out[None]


def solution(mesh):
    tok = P("dp", "sp", None)
    exp = P(("sp", "dp"), None, None)
    in_specs = (
        tok, tok, tok, P(), P(), P(), P(), tok, P(), tok, tok, exp, exp, exp,
    )
    return jax.shard_map(
        local, mesh=mesh, in_specs=in_specs, out_specs=(tok, tok), check_vma=False
    )
```

```python
import numpy as np
import jax
import jax.numpy as jnp
from jax import lax
from jax.experimental import pallas as pl
from jax.experimental.pallas import tpu as pltpu
from jax.sharding import PartitionSpec as P

D = 2048
HEADS = 32
PLAIN = 64
ROT = 32
QK = PLAIN + ROT
LAT = 256
TOPK = 2
GRID_W = 64
FF = 1024
CAP = 4
GROUP = 4
CHUNK = 256
F_STEPS = 1
O_STEPS = 2
PER = 1
EPS = 1e-06
CLAMP = 7.0
ALPHA = 1.702
LOG2E = 1.4426950408889634
BF = jnp.bfloat16
F32 = jnp.float32


def prep_kernel(
    off_ref, lat_ref, rope_ref, gain_ref, freq_ref, out_ref, cos_ref, sin_ref
):
    toks = lat_ref.shape[0]
    p = off_ref[0] * toks + lax.broadcasted_iota(jnp.int32, (ROT, toks), 1)
    entry = lax.broadcasted_iota(jnp.int32, (ROT, toks), 0)
    place = jnp.where(entry < ROT // 2, p // GRID_W, p % GRID_W).astype(F32)
    angle = place * freq_ref[...]
    cosine = jnp.cos(angle)
    sine = jnp.where(entry % 2 == 0, -jnp.sin(angle), jnp.sin(angle))
    cos_ref[...] = cosine
    sin_ref[...] = sine
    lat = lat_ref[...].astype(F32)
    ms = jnp.mean(lat * lat, axis=-1, keepdims=True)
    latent = lat * lax.rsqrt(ms + EPS) * gain_ref[...]
    turned = turn(rope_ref[...].astype(F32), cosine, sine)
    both = jnp.concatenate([latent.T, turned], axis=0).astype(BF)
    for i in range(out_ref.shape[0]):
        out_ref[i] = both


def turn(x, cosine, sine):
    y = x.reshape(x.shape[0] // 8, 8, x.shape[1])
    even = lax.broadcasted_iota(jnp.int32, y.shape, 1) % 2 == 0
    swapped = jnp.where(even, pltpu.roll(y, 7, 1), pltpu.roll(y, 1, 1)).reshape(x.shape)
    return x * cosine + swapped * sine


def pair_frequencies():
    pair = np.arange(ROT) // 2 % (ROT // 4)
    return (10000.0 ** (-(2.0 * pair) / (ROT // 2))).astype(np.float32)[:, None]


def route_kernel(col_ref, row_ref, weight_ref, bcol_ref, brow_ref, wcol_ref):
    wcol_ref[...] = weight_ref[...]
    n = col_ref.shape[0]
    sub = lax.broadcasted_iota(jnp.int32, (n, n), 0)
    lane = lax.broadcasted_iota(jnp.int32, (n, n), 1)
    e_c = [col_ref[:, k : k + 1] for k in range(2)]
    e_r = [row_ref[k : k + 1, :] for k in range(2)]
    same00 = e_c[0] == e_r[0]
    same11 = e_c[1] == e_r[1]
    one = lambda m: jnp.where(m, 1.0, 0.0)
    r0 = jnp.sum(one(same00 & (lane < sub)), axis=1, keepdims=True)
    r1 = jnp.sum(one(same11 & (lane < sub)), axis=1, keepdims=True) + jnp.sum(
        one(e_c[1] == e_r[0]), axis=1, keepdims=True
    )
    bcol_ref[:, 0:1] = e_c[0] * 8 + r0.astype(jnp.int32)
    bcol_ref[:, 1:2] = e_c[1] * 8 + r1.astype(jnp.int32)
    s0 = jnp.sum(one(same00 & (sub < lane)), axis=0, keepdims=True)
    s1 = jnp.sum(one(same11 & (sub < lane)), axis=0, keepdims=True) + jnp.sum(
        one(e_c[0] == e_r[1]), axis=0, keepdims=True
    )
    brow_ref[0:1, :] = e_r[0] * 8 + s0.astype(jnp.int32)
    brow_ref[1:2, :] = e_r[1] * 8 + s1.astype(jnp.int32)


def dot(a, b, dims):
    return lax.dot_general(a, b, (dims, ((), ())), preferred_element_type=F32)


def query_kernel(q_ref, cos_ref, sin_ref, ku_ref, out_ref, bd_ref):
    toks = q_ref.shape[0]

    @pl.when(pl.program_id(0) == 0)
    def _():
        bd_ref[...] = jnp.zeros_like(bd_ref)

    qt = q_ref[...].astype(F32).T * (QK ** -0.5)
    for j in range(GROUP):
        bd_ref[j * PLAIN : (j + 1) * PLAIN, j * toks : (j + 1) * toks] = qt[
            j * QK : j * QK + PLAIN
        ].astype(BF)
    out_ref[0, :LAT, :] = (dot(ku_ref[...], bd_ref[...], ((1,), (0,))) * LOG2E).astype(BF)
    for j in range(GROUP):
        r = j * QK + PLAIN
        turned = turn(qt[r : r + ROT], cos_ref[...], sin_ref[...])
        out_ref[0, LAT:, j * toks : (j + 1) * toks] = (turned * LOG2E).astype(BF)


def attend_kernel(
    kt_ref, q_ref, vb_ref, va_ref, vl_ref, w_hbm, res_ref, gain_ref, brow_ref, mixed_ref, normed_ref, out_ref,
    keys_ref, klt_ref, sa_ref, sb_ref, pa_ref, pb_ref, ta_ref, lb_ref, acc_ref, w_ref, sem_ref,
):
    g = pl.program_id(0)
    parts = (pl.ds(0, GROUP * PLAIN), pl.ds(GROUP * PLAIN, D - GROUP * PLAIN))
    w_first, w_rest = [
        pltpu.make_async_copy(w_hbm.at[part], w_ref.at[part], sem_ref.at[i])
        for i, part in enumerate(parts)
    ]
    last = pl.num_programs(0) - 1
    toks = res_ref.shape[0]
    n_keys = keys_ref.shape[0]
    chunk = CHUNK
    chunks = n_keys // chunk

    def pieces(x):
        return x.reshape(x.shape[0] // 8, 8, x.shape[1])

    def score_chunk(q, s_ref, i, top):
        rows = slice(i * chunk, (i + 1) * chunk)
        s = dot(keys_ref[rows, :], q, ((1,), (0,)))
        s_ref[rows, :] = s
        part = jnp.max(pieces(s), axis=0)
        return part if top is None else jnp.maximum(top, part)

    def prob_chunk(s_ref, p_ref, i, top, total):
        rows = slice(i * chunk, (i + 1) * chunk)
        p = jnp.exp2(s_ref[rows, :] - top)
        p_ref[rows, :] = p.astype(BF)
        part = jnp.sum(pieces(p), axis=0)
        return part if total is None else total + part

    def context(p_ref, total):
        ctx = dot(klt_ref[...], p_ref[...], ((1,), (0,)))
        return (ctx * (1.0 / jnp.sum(total, axis=0, keepdims=True))).astype(BF)

    def rows_of(group):
        return pl.ds(pl.multiple_of(group * GROUP * PLAIN, GROUP * PLAIN), GROUP * PLAIN)

    def heads_of(ctx, v_ref):
        full_out = dot(v_ref[...], ctx, ((1,), (0,)))
        own = [
            full_out[j * PLAIN : (j + 1) * PLAIN, j * toks : (j + 1) * toks] for j in range(GROUP)
        ]
        return jnp.concatenate(own, axis=0).astype(BF)

    def project(heads, group):
        acc_ref[...] += dot(heads, w_ref[rows_of(group), :], ((0,), (0,)))

    def stage(after, s_new, s_old, p_new, p_old, top_old, total_old, v_ref, group):
        top, total, ctx, heads = None, None, None, None
        for i in range(chunks):
            if after is not None:
                top = score_chunk(q_ref[after], s_new, i, top)
            total = prob_chunk(s_old, p_new, i, top_old, total)
            if i == chunks // 8:
                ctx = context(p_old, total_old)
            if i == chunks // 2:
                heads = heads_of(ctx, v_ref)
            if i == chunks * 3 // 4:
                project(heads, group)
        if after is not None:
            top = jnp.max(top, axis=0, keepdims=True)
        return top, total

    @pl.when(g == 0)
    def _():
        w_first.start()
        w_rest.start()
        for i in range(kt_ref.shape[0]):
            rows = slice(i * toks, (i + 1) * toks)
            klt_ref[:, rows] = kt_ref[i, :LAT, :]
            keys_ref[rows, :] = kt_ref[i].T
        top = None
        for i in range(chunks):
            top = score_chunk(q_ref[0], sa_ref, i, top)
        ta_ref[...] = jnp.max(top, axis=0, keepdims=True)
        w_first.wait()

    top_b, total_a = stage(
        2 * g + 1, sb_ref, sa_ref, pa_ref, pb_ref, ta_ref[...], lb_ref[...], vb_ref,
        jnp.maximum(2 * g - 1, 0),
    )

    @pl.when(g == 0)
    def _():
        w_rest.wait()
        acc_ref[...] = res_ref[...].astype(F32)

    @pl.when(g < last)
    def _():
        top_a, total_b = stage(
            2 * g + 2, sa_ref, sb_ref, pb_ref, pa_ref, top_b, total_a, va_ref, 2 * g
        )
        ta_ref[...] = top_a
        lb_ref[...] = total_b

    @pl.when(g == last)
    def _():
        _, total_b = stage(None, sa_ref, sb_ref, pb_ref, pa_ref, top_b, total_a, va_ref, 2 * g)
        project(heads_of(context(pb_ref, total_b), vl_ref), 2 * g + 1)
        mixed = acc_ref[...]
        mixed_ref[...] = mixed
        ms = jnp.mean(mixed * mixed, axis=-1, keepdims=True)
        normed = (mixed * lax.rsqrt(ms + EPS) * gain_ref[...]).astype(BF)
        normed_ref[...] = normed
        n_rows = out_ref.shape[0]
        half_d = D // 2
        stacked = jnp.concatenate([normed[:, :half_d], normed[:, half_d:]], axis=0)
        row = lax.broadcasted_iota(jnp.int32, (n_rows, toks), 0)
        picks = []
        for h in range(2):
            m = (row == brow_ref[0:1, :] + 4 * h) | (row == brow_ref[1:2, :] + 4 * h)
            picks.append(jnp.where(m, 1.0, 0.0).astype(BF))
        pick = jnp.concatenate(picks, axis=1)
        out_ref[...] = dot(pick, stacked, ((1,), (0,))).astype(BF)


def expert_kernel(
    rows_ref, gate_ref, up_hbm, down_hbm, out_ref, x_ref, hidden_ref, up_ref, down_ref, sem_ref
):
    f = pl.program_id(0)
    copy_up = pltpu.make_async_copy(up_hbm, up_ref, sem_ref.at[0])
    copy_down = pltpu.make_async_copy(down_hbm, down_ref, sem_ref.at[1])
    n_src = rows_ref.shape[0]
    half_d = D // 2
    f_steps, _, fb = hidden_ref.shape
    lanes = out_ref.shape[2]

    @pl.when(f == 0)
    def _():
        copy_up.start()
        copy_down.start()
        r = rows_ref[...].astype(F32).reshape(n_src // 2, 2, 8, half_d)
        a, b = r[:, 0], r[:, 1]
        low = lax.broadcasted_iota(jnp.int32, a.shape, 1) < 4
        first = jnp.where(low, a, pltpu.roll(b, 4, 1))
        second = jnp.where(low, pltpu.roll(a, 4, 1), b)
        x_ref[:, :half_d] = first.reshape(n_src * 4, half_d).astype(BF)
        x_ref[:, half_d:] = second.reshape(n_src * 4, half_d).astype(BF)

    @pl.when(f == 0)
    def _():
        copy_up.wait()

    @pl.when(f == f_steps)
    def _():
        copy_down.wait()

    @pl.when(f < f_steps)
    def _():
        x = x_ref[...]
        cols = pl.ds(pl.multiple_of(f * fb, fb), fb)
        gate = dot(x, gate_ref[:, cols], ((1,), (0,)))
        up = dot(x, up_ref[:, cols], ((1,), (0,)))
        cut = jnp.minimum(gate, CLAMP)
        act = cut * jax.nn.sigmoid(ALPHA * cut) * (jnp.clip(up, -CLAMP, CLAMP) + 1.0)
        hidden_ref[f] = act.astype(BF)

    @pl.when(f >= f_steps)
    def _():
        hidden = jnp.concatenate([hidden_ref[i] for i in range(f_steps)], axis=1)
        at = pl.multiple_of((f - f_steps) * lanes, lanes)
        lo = dot(hidden, down_ref[:, pl.ds(at, lanes)], ((1,), (0,)))
        hi = dot(hidden, down_ref[:, pl.ds(at + half_d, lanes)], ((1,), (0,)))
        lo = lo.reshape(n_src // 2, 8, lanes)
        hi = hi.reshape(n_src // 2, 8, lanes)
        low = lax.broadcasted_iota(jnp.int32, lo.shape, 1) < 4
        first = jnp.where(low, lo, pltpu.roll(hi, 4, 1))
        second = jnp.where(low, pltpu.roll(lo, 4, 1), hi)
        both = jnp.concatenate([first[:, None], second[:, None]], axis=1)
        out_ref[...] = both.reshape(n_src, 8, lanes).astype(BF)


def combine_kernel(rows_ref, bcol_ref, weight_ref, mixed_ref, out_ref, pick_ref):
    n = pl.program_id(0)
    n_rows = rows_ref.shape[0]
    toks = mixed_ref.shape[0]
    per = pl.num_programs(0) // 2

    @pl.when(n % per == 0)
    def _():
        lane = lax.broadcasted_iota(jnp.int32, (toks, n_rows), 1)
        shift = 4 * (n // per)
        for k in range(TOPK):
            pick = jnp.where(lane == bcol_ref[:, k : k + 1] + shift, 1.0, 0.0).astype(BF)
            pick_ref[k * toks : (k + 1) * toks, :] = pick

    lanes = mixed_ref.shape[1]
    cols = pl.ds(pl.multiple_of(n % per * lanes, lanes), lanes)
    got = dot(pick_ref[...], rows_ref[:, cols], ((1,), (0,)))
    total = mixed_ref[...]
    for k in range(TOPK):
        total += weight_ref[:, k : k + 1] * got[k * toks : (k + 1) * toks]
    out_ref[...] = total.astype(BF)


def in_vmem(x):
    return pltpu.with_memory_space_constraint(x, pltpu.VMEM)


def in_hbm(x):
    return pltpu.with_memory_space_constraint(x, pltpu.HBM)


def whole():
    return pl.BlockSpec(memory_space=pltpu.VMEM)


def full(*shape):
    return pl.BlockSpec(shape, lambda *_: (0,) * len(shape))


def params(mb=60):
    return pltpu.CompilerParams(vmem_limit_bytes=mb * 1024 * 1024)


def ready_queries(q, ct, st, ku):
    toks = q.shape[0]
    return pl.pallas_call(
        query_kernel,
        grid=(HEADS // GROUP,),
        in_specs=[
            pl.BlockSpec((toks, GROUP * QK), lambda g: (0, g)),
            full(ROT, toks),
            full(ROT, toks),
            pl.BlockSpec((LAT, GROUP * PLAIN), lambda g: (0, g)),
        ],
        out_specs=pl.BlockSpec((1, LAT + ROT, GROUP * toks), lambda g: (g, 0, 0)),
        out_shape=jax.ShapeDtypeStruct((HEADS // GROUP, LAT + ROT, GROUP * toks), BF),
        scratch_shapes=[pltpu.VMEM((GROUP * PLAIN, GROUP * toks), BF)],
        compiler_params=params(24),
        name="queries",
    )(q, ct, st, ku)


def attend(qs, keys, vut, wo, res, gain, brow, experts):
    sds = jax.ShapeDtypeStruct
    toks = res.shape[0]
    keys_n = keys.shape[0] * toks
    groups = HEADS // GROUP
    v_at = lambda f: pl.BlockSpec((GROUP * PLAIN, LAT), lambda g: (f(g), 0))
    return pl.pallas_call(
        attend_kernel,
        grid=(groups // 2,),
        in_specs=[
            whole(),
            whole(),
            v_at(lambda g: jnp.maximum(2 * g - 1, 0)),
            v_at(lambda g: 2 * g),
            v_at(lambda g: groups - 1),
            pl.BlockSpec(memory_space=pl.ANY),
            full(toks, D),
            full(1, D),
            full(TOPK, toks),
        ],
        out_specs=(full(toks, D), full(toks, D), full(experts * 8, D // 2)),
        out_shape=(sds((toks, D), F32), sds((toks, D), BF), sds((experts * 8, D // 2), BF)),
        scratch_shapes=[
            pltpu.VMEM((keys_n, LAT + ROT), BF),
            pltpu.VMEM((LAT, keys_n), BF),
            pltpu.VMEM((keys_n, GROUP * toks), F32),
            pltpu.VMEM((keys_n, GROUP * toks), F32),
            pltpu.VMEM((keys_n, GROUP * toks), BF),
            pltpu.VMEM((keys_n, GROUP * toks), BF),
            pltpu.VMEM((1, GROUP * toks), F32),
            pltpu.VMEM((8, GROUP * toks), F32),
            pltpu.VMEM((toks, D), F32),
            pltpu.VMEM((D, D), BF),
            pltpu.SemaphoreType.DMA((2,)),
        ],
        compiler_params=params(44),
        name="attend",
    )(keys, in_vmem(qs), vut, vut, vut, in_hbm(wo), res, in_hbm(gain), in_hbm(brow))


def run_experts(slot_rows, gate, up, down, f_steps, o_steps):
    sds = jax.ShapeDtypeStruct
    experts = slot_rows.shape[0]
    fb, lanes = FF // f_steps, D // 2 // o_steps
    out_at = lambda f: jnp.maximum(f - f_steps, 0)
    return pl.pallas_call(
        expert_kernel,
        grid=(f_steps + o_steps,),
        in_specs=[whole()] * 2 + [pl.BlockSpec(memory_space=pl.ANY)] * 2,
        out_specs=pl.BlockSpec((experts, 8, lanes), lambda f: (0, 0, out_at(f))),
        out_shape=sds((experts, 8, D // 2), BF),
        scratch_shapes=[
            pltpu.VMEM((experts * CAP, D), BF),
            pltpu.VMEM((f_steps, experts * CAP, fb), BF),
            pltpu.VMEM((D, FF), BF),
            pltpu.VMEM((FF, D), BF),
            pltpu.SemaphoreType.DMA((2,)),
        ],
        compiler_params=params(40),
        name="experts",
    )(
        in_vmem(slot_rows),
        in_vmem(gate),
        up,
        down,
    )


def run_combine(rows, bcol, wcol, mixed, per):
    toks = mixed.shape[0]
    n_rows = rows.shape[0]
    return pl.pallas_call(
        combine_kernel,
        grid=(2 * per,),
        in_specs=[
            whole(),
            full(toks, TOPK),
            full(toks, TOPK),
            pl.BlockSpec((toks, D // 2 // per), lambda n: (0, n)),
        ],
        out_specs=pl.BlockSpec((toks, D // 2 // per), lambda n: (0, n)),
        out_shape=jax.ShapeDtypeStruct((toks, D), BF),
        scratch_shapes=[pltpu.VMEM((TOPK * toks, n_rows), BF)],
        compiler_params=params(40),
        name="combine",
    )(in_vmem(rows), bcol, wcol, mixed)


def local(
    queries, kv_latent, rope_key, latent_norm_gain, key_up_weight, value_up_weight, out_proj,
    residual, ffn_gain, routes, route_weights, expert_gate, expert_up, expert_down,
):
    toks = queries.shape[1]
    sp = lax.axis_size("sp")
    experts = sp * lax.axis_size("dp")
    sds = jax.ShapeDtypeStruct
    offset = lax.axis_index("sp").astype(jnp.int32)[None]
    packed, ct, st = pl.pallas_call(
        prep_kernel,
        in_specs=[pl.BlockSpec(memory_space=pltpu.SMEM)] + [pl.BlockSpec()] * 4,
        out_shape=(sds((sp, LAT + ROT, toks), BF), sds((ROT, toks), F32), sds((ROT, toks), F32)),
        compiler_params=params(),
        name="prep",
    )(offset, kv_latent[0], rope_key[0].T, latent_norm_gain[None], pair_frequencies())
    keys = in_vmem(lax.all_to_all(packed, "sp", 0, 0, tiled=True))
    bcol, brow, wcol = pl.pallas_call(
        route_kernel,
        out_shape=(
            sds((toks, TOPK), jnp.int32), sds((TOPK, toks), jnp.int32), sds((toks, TOPK), F32)
        ),
        compiler_params=params(),
        name="routes",
    )(routes[0], routes[0].T, route_weights[0])

    mixed, normed, outgoing = attend(
        ready_queries(queries[0], ct, st, key_up_weight), keys, value_up_weight.T, out_proj,
        in_hbm(residual[0]), ffn_gain[None], brow, experts,
    )

    slot_rows = lax.all_to_all(
        outgoing.reshape(experts, 8, D // 2), ("sp", "dp"), 0, 0, tiled=True
    )
    expert_out = run_experts(
        slot_rows, expert_gate[0], expert_up[0], expert_down[0], F_STEPS, O_STEPS
    )
    returned = lax.all_to_all(expert_out, ("sp", "dp"), 0, 0, tiled=True)
    layer_out = run_combine(returned.reshape(experts * 8, D // 2), bcol, wcol, mixed, PER)
    return normed[None], layer_out[None]


def solution(mesh):
    tok = P("dp", "sp", None)
    exp = P(("sp", "dp"), None, None)
    in_specs = (
        tok, tok, tok, P(), P(), P(), P(), tok, P(), tok, tok, exp, exp, exp,
    )
    return jax.shard_map(
        local, mesh=mesh, in_specs=in_specs, out_specs=(tok, tok), check_vma=False
    )
```

```python
import numpy as np
import jax
import jax.numpy as jnp
from jax import lax
from jax.experimental import pallas as pl
from jax.experimental.pallas import tpu as pltpu
from jax.sharding import PartitionSpec as P

D = 2048
HEADS = 32
PLAIN = 64
ROT = 32
QK = PLAIN + ROT
LAT = 256
TOPK = 2
GRID_W = 64
FF = 1024
CAP = 4
GROUP = 4
CHUNK = 256
F_STEPS = 1
O_STEPS = 2
PER = 1
EPS = 1e-06
CLAMP = 7.0
ALPHA = 1.702
LOG2E = 1.4426950408889634
BF = jnp.bfloat16
F32 = jnp.float32


def prep_kernel(
    off_ref, lat_ref, rope_ref, gain_ref, freq_ref, out_ref, cos_ref, sin_ref
):
    toks = lat_ref.shape[0]
    p = off_ref[0] * toks + lax.broadcasted_iota(jnp.int32, (ROT, toks), 1)
    entry = lax.broadcasted_iota(jnp.int32, (ROT, toks), 0)
    place = jnp.where(entry < ROT // 2, p // GRID_W, p % GRID_W).astype(F32)
    angle = place * freq_ref[...]
    cosine = jnp.cos(angle)
    sine = jnp.where(entry % 2 == 0, -jnp.sin(angle), jnp.sin(angle))
    cos_ref[...] = cosine
    sin_ref[...] = sine
    lat = lat_ref[...].astype(F32)
    ms = jnp.mean(lat * lat, axis=-1, keepdims=True)
    latent = lat * lax.rsqrt(ms + EPS) * gain_ref[...]
    turned = turn(rope_ref[...].astype(F32), cosine, sine)
    both = jnp.concatenate([latent.T, turned], axis=0).astype(BF)
    for i in range(out_ref.shape[0]):
        out_ref[i] = both


def turn(x, cosine, sine):
    y = x.reshape(x.shape[0] // 8, 8, x.shape[1])
    even = lax.broadcasted_iota(jnp.int32, y.shape, 1) % 2 == 0
    swapped = jnp.where(even, pltpu.roll(y, 7, 1), pltpu.roll(y, 1, 1)).reshape(x.shape)
    return x * cosine + swapped * sine


def pair_frequencies():
    pair = np.arange(ROT) // 2 % (ROT // 4)
    return (10000.0 ** (-(2.0 * pair) / (ROT // 2))).astype(np.float32)[:, None]


def route_kernel(col_ref, row_ref, weight_ref, bcol_ref, brow_ref, wcol_ref):
    wcol_ref[...] = weight_ref[...]
    n = col_ref.shape[0]
    sub = lax.broadcasted_iota(jnp.int32, (n, n), 0)
    lane = lax.broadcasted_iota(jnp.int32, (n, n), 1)
    e_c = [col_ref[:, k : k + 1] for k in range(2)]
    e_r = [row_ref[k : k + 1, :] for k in range(2)]
    same00 = e_c[0] == e_r[0]
    same11 = e_c[1] == e_r[1]
    one = lambda m: jnp.where(m, 1.0, 0.0)
    r0 = jnp.sum(one(same00 & (lane < sub)), axis=1, keepdims=True)
    r1 = jnp.sum(one(same11 & (lane < sub)), axis=1, keepdims=True) + jnp.sum(
        one(e_c[1] == e_r[0]), axis=1, keepdims=True
    )
    bcol_ref[:, 0:1] = e_c[0] * 8 + r0.astype(jnp.int32)
    bcol_ref[:, 1:2] = e_c[1] * 8 + r1.astype(jnp.int32)
    s0 = jnp.sum(one(same00 & (sub < lane)), axis=0, keepdims=True)
    s1 = jnp.sum(one(same11 & (sub < lane)), axis=0, keepdims=True) + jnp.sum(
        one(e_c[0] == e_r[1]), axis=0, keepdims=True
    )
    brow_ref[0:1, :] = e_r[0] * 8 + s0.astype(jnp.int32)
    brow_ref[1:2, :] = e_r[1] * 8 + s1.astype(jnp.int32)


def dot(a, b, dims):
    return lax.dot_general(a, b, (dims, ((), ())), preferred_element_type=F32)


def query_kernel(q_ref, cos_ref, sin_ref, ku_ref, out_ref, bd_ref):
    toks = q_ref.shape[0]

    @pl.when(pl.program_id(0) == 0)
    def _():
        bd_ref[...] = jnp.zeros_like(bd_ref)

    qt = q_ref[...].astype(F32).T * (QK ** -0.5)
    for j in range(GROUP):
        bd_ref[j * PLAIN : (j + 1) * PLAIN, j * toks : (j + 1) * toks] = qt[
            j * QK : j * QK + PLAIN
        ].astype(BF)
    out_ref[0, :LAT, :] = (dot(ku_ref[...], bd_ref[...], ((1,), (0,))) * LOG2E).astype(BF)
    for j in range(GROUP):
        r = j * QK + PLAIN
        turned = turn(qt[r : r + ROT], cos_ref[...], sin_ref[...])
        out_ref[0, LAT:, j * toks : (j + 1) * toks] = (turned * LOG2E).astype(BF)


def attend_kernel(
    kt_ref, q_ref, vb_ref, va_ref, vl_ref, w_hbm, res_ref, gain_ref, brow_ref, mixed_ref, normed_ref, out_ref,
    keys_ref, klt_ref, sa_ref, sb_ref, pa_ref, pb_ref, ta_ref, lb_ref, acc_ref, w_ref, sem_ref,
):
    g = pl.program_id(0)
    parts = (pl.ds(0, GROUP * PLAIN), pl.ds(GROUP * PLAIN, D - GROUP * PLAIN))
    w_first, w_rest = [
        pltpu.make_async_copy(w_hbm.at[part], w_ref.at[part], sem_ref.at[i])
        for i, part in enumerate(parts)
    ]
    last = pl.num_programs(0) - 1
    toks = res_ref.shape[0]
    n_keys = keys_ref.shape[0]
    chunk = CHUNK
    chunks = n_keys // chunk

    def pieces(x):
        return x.reshape(x.shape[0] // 8, 8, x.shape[1])

    def score_chunk(q, s_ref, i, top):
        rows = slice(i * chunk, (i + 1) * chunk)
        s = dot(keys_ref[rows, :], q, ((1,), (0,)))
        s_ref[rows, :] = s
        part = jnp.max(pieces(s), axis=0)
        return part if top is None else jnp.maximum(top, part)

    def prob_chunk(s_ref, p_ref, i, top, total):
        rows = slice(i * chunk, (i + 1) * chunk)
        p = jnp.exp2(s_ref[rows, :] - top)
        p_ref[rows, :] = p.astype(BF)
        part = jnp.sum(pieces(p), axis=0)
        return part if total is None else total + part

    def context(p_ref, total):
        ctx = dot(klt_ref[...], p_ref[...], ((1,), (0,)))
        return (ctx * (1.0 / jnp.sum(total, axis=0, keepdims=True))).astype(BF)

    def rows_of(group):
        return pl.ds(pl.multiple_of(group * GROUP * PLAIN, GROUP * PLAIN), GROUP * PLAIN)

    def heads_of(ctx, v_ref):
        full_out = dot(v_ref[...], ctx, ((1,), (0,)))
        own = [
            full_out[j * PLAIN : (j + 1) * PLAIN, j * toks : (j + 1) * toks] for j in range(GROUP)
        ]
        return jnp.concatenate(own, axis=0).astype(BF)

    def project(heads, group):
        acc_ref[...] += dot(heads, w_ref[rows_of(group), :], ((0,), (0,)))

    def stage(after, s_new, s_old, p_new, p_old, top_old, total_old, v_ref, group):
        top, total, ctx, heads = None, None, None, None
        for i in range(chunks):
            if after is not None:
                top = score_chunk(q_ref[after], s_new, i, top)
            total = prob_chunk(s_old, p_new, i, top_old, total)
            if i == chunks // 8:
                ctx = context(p_old, total_old)
            if i == chunks // 2:
                heads = heads_of(ctx, v_ref)
            if i == chunks * 3 // 4:
                project(heads, group)
        if after is not None:
            top = jnp.max(top, axis=0, keepdims=True)
        return top, total

    @pl.when(g == 0)
    def _():
        w_first.start()
        w_rest.start()
        for i in range(kt_ref.shape[0]):
            rows = slice(i * toks, (i + 1) * toks)
            klt_ref[:, rows] = kt_ref[i, :LAT, :]
            keys_ref[rows, :] = kt_ref[i].T
        top = None
        for i in range(chunks):
            top = score_chunk(q_ref[0], sa_ref, i, top)
        ta_ref[...] = jnp.max(top, axis=0, keepdims=True)
        w_first.wait()

    top_b, total_a = stage(
        2 * g + 1, sb_ref, sa_ref, pa_ref, pb_ref, ta_ref[...], lb_ref[...], vb_ref,
        jnp.maximum(2 * g - 1, 0),
    )

    @pl.when(g == 0)
    def _():
        w_rest.wait()
        acc_ref[...] = res_ref[...].astype(F32)

    @pl.when(g < last)
    def _():
        top_a, total_b = stage(
            2 * g + 2, sa_ref, sb_ref, pb_ref, pa_ref, top_b, total_a, va_ref, 2 * g
        )
        ta_ref[...] = top_a
        lb_ref[...] = total_b

    @pl.when(g == last)
    def _():
        _, total_b = stage(None, sa_ref, sb_ref, pb_ref, pa_ref, top_b, total_a, va_ref, 2 * g)
        project(heads_of(context(pb_ref, total_b), vl_ref), 2 * g + 1)
        mixed = acc_ref[...]
        mixed_ref[...] = mixed
        ms = jnp.mean(mixed * mixed, axis=-1, keepdims=True)
        normed = (mixed * lax.rsqrt(ms + EPS) * gain_ref[...]).astype(BF)
        normed_ref[...] = normed
        n_rows = out_ref.shape[0]
        half_d = D // 2
        stacked = jnp.concatenate([normed[:, :half_d], normed[:, half_d:]], axis=0)
        row = lax.broadcasted_iota(jnp.int32, (n_rows, toks), 0)
        picks = []
        for h in range(2):
            m = (row == brow_ref[0:1, :] + 4 * h) | (row == brow_ref[1:2, :] + 4 * h)
            picks.append(jnp.where(m, 1.0, 0.0).astype(BF))
        pick = jnp.concatenate(picks, axis=1)
        out_ref[...] = dot(pick, stacked, ((1,), (0,))).astype(BF)


def expert_kernel(
    rows_ref, gate_ref, up_ref, down_hbm, out_ref, x_ref, hidden_ref, down_ref, sem_ref
):
    f = pl.program_id(0)
    copy_down = pltpu.make_async_copy(down_hbm, down_ref, sem_ref.at[0])
    n_src = rows_ref.shape[0]
    half_d = D // 2
    f_steps, _, fb = hidden_ref.shape
    lanes = out_ref.shape[2]

    @pl.when(f == 0)
    def _():
        copy_down.start()
        r = rows_ref[...].astype(F32).reshape(n_src // 2, 2, 8, half_d)
        a, b = r[:, 0], r[:, 1]
        low = lax.broadcasted_iota(jnp.int32, a.shape, 1) < 4
        first = jnp.where(low, a, pltpu.roll(b, 4, 1))
        second = jnp.where(low, pltpu.roll(a, 4, 1), b)
        x_ref[:, :half_d] = first.reshape(n_src * 4, half_d).astype(BF)
        x_ref[:, half_d:] = second.reshape(n_src * 4, half_d).astype(BF)

    @pl.when(f == f_steps)
    def _():
        copy_down.wait()

    @pl.when(f < f_steps)
    def _():
        x = x_ref[...]
        cols = pl.ds(pl.multiple_of(f * fb, fb), fb)
        gate = dot(x, gate_ref[:, cols], ((1,), (0,)))
        up = dot(x, up_ref[:, cols], ((1,), (0,)))
        cut = jnp.minimum(gate, CLAMP)
        act = cut * jax.nn.sigmoid(ALPHA * cut) * (jnp.clip(up, -CLAMP, CLAMP) + 1.0)
        hidden_ref[f] = act.astype(BF)

    @pl.when(f >= f_steps)
    def _():
        hidden = jnp.concatenate([hidden_ref[i] for i in range(f_steps)], axis=1)
        at = pl.multiple_of((f - f_steps) * lanes, lanes)
        lo = dot(hidden, down_ref[:, pl.ds(at, lanes)], ((1,), (0,)))
        hi = dot(hidden, down_ref[:, pl.ds(at + half_d, lanes)], ((1,), (0,)))
        lo = lo.reshape(n_src // 2, 8, lanes)
        hi = hi.reshape(n_src // 2, 8, lanes)
        low = lax.broadcasted_iota(jnp.int32, lo.shape, 1) < 4
        first = jnp.where(low, lo, pltpu.roll(hi, 4, 1))
        second = jnp.where(low, pltpu.roll(lo, 4, 1), hi)
        both = jnp.concatenate([first[:, None], second[:, None]], axis=1)
        out_ref[...] = both.reshape(n_src, 8, lanes).astype(BF)


def combine_kernel(rows_ref, bcol_ref, weight_ref, mixed_ref, out_ref, pick_ref):
    n = pl.program_id(0)
    n_rows = rows_ref.shape[0]
    toks = mixed_ref.shape[0]
    per = pl.num_programs(0) // 2

    @pl.when(n % per == 0)
    def _():
        lane = lax.broadcasted_iota(jnp.int32, (toks, n_rows), 1)
        shift = 4 * (n // per)
        for k in range(TOPK):
            pick = jnp.where(lane == bcol_ref[:, k : k + 1] + shift, 1.0, 0.0).astype(BF)
            pick_ref[k * toks : (k + 1) * toks, :] = pick

    lanes = mixed_ref.shape[1]
    cols = pl.ds(pl.multiple_of(n % per * lanes, lanes), lanes)
    got = dot(pick_ref[...], rows_ref[:, cols], ((1,), (0,)))
    total = mixed_ref[...]
    for k in range(TOPK):
        total += weight_ref[:, k : k + 1] * got[k * toks : (k + 1) * toks]
    out_ref[...] = total.astype(BF)


def in_vmem(x):
    return pltpu.with_memory_space_constraint(x, pltpu.VMEM)


def in_hbm(x):
    return pltpu.with_memory_space_constraint(x, pltpu.HBM)


def whole():
    return pl.BlockSpec(memory_space=pltpu.VMEM)


def full(*shape):
    return pl.BlockSpec(shape, lambda *_: (0,) * len(shape))


def params(mb=60):
    return pltpu.CompilerParams(vmem_limit_bytes=mb * 1024 * 1024)


def ready_queries(q, ct, st, ku):
    toks = q.shape[0]
    return pl.pallas_call(
        query_kernel,
        grid=(HEADS // GROUP,),
        in_specs=[
            pl.BlockSpec((toks, GROUP * QK), lambda g: (0, g)),
            full(ROT, toks),
            full(ROT, toks),
            pl.BlockSpec((LAT, GROUP * PLAIN), lambda g: (0, g)),
        ],
        out_specs=pl.BlockSpec((1, LAT + ROT, GROUP * toks), lambda g: (g, 0, 0)),
        out_shape=jax.ShapeDtypeStruct((HEADS // GROUP, LAT + ROT, GROUP * toks), BF),
        scratch_shapes=[pltpu.VMEM((GROUP * PLAIN, GROUP * toks), BF)],
        compiler_params=params(24),
        name="queries",
    )(q, ct, st, ku)


def attend(qs, keys, vut, wo, res, gain, brow, experts):
    sds = jax.ShapeDtypeStruct
    toks = res.shape[0]
    keys_n = keys.shape[0] * toks
    groups = HEADS // GROUP
    v_at = lambda f: pl.BlockSpec((GROUP * PLAIN, LAT), lambda g: (f(g), 0))
    return pl.pallas_call(
        attend_kernel,
        grid=(groups // 2,),
        in_specs=[
            whole(),
            whole(),
            v_at(lambda g: jnp.maximum(2 * g - 1, 0)),
            v_at(lambda g: 2 * g),
            v_at(lambda g: groups - 1),
            pl.BlockSpec(memory_space=pl.ANY),
            full(toks, D),
            full(1, D),
            full(TOPK, toks),
        ],
        out_specs=(full(toks, D), full(toks, D), full(experts * 8, D // 2)),
        out_shape=(sds((toks, D), F32), sds((toks, D), BF), sds((experts * 8, D // 2), BF)),
        scratch_shapes=[
            pltpu.VMEM((keys_n, LAT + ROT), BF),
            pltpu.VMEM((LAT, keys_n), BF),
            pltpu.VMEM((keys_n, GROUP * toks), F32),
            pltpu.VMEM((keys_n, GROUP * toks), F32),
            pltpu.VMEM((keys_n, GROUP * toks), BF),
            pltpu.VMEM((keys_n, GROUP * toks), BF),
            pltpu.VMEM((1, GROUP * toks), F32),
            pltpu.VMEM((8, GROUP * toks), F32),
            pltpu.VMEM((toks, D), F32),
            pltpu.VMEM((D, D), BF),
            pltpu.SemaphoreType.DMA((2,)),
        ],
        compiler_params=params(44),
        name="attend",
    )(keys, in_vmem(qs), vut, vut, vut, in_hbm(wo), res, in_hbm(gain), in_hbm(brow))


def run_experts(slot_rows, gate, up, down, f_steps, o_steps):
    sds = jax.ShapeDtypeStruct
    experts = slot_rows.shape[0]
    fb, lanes = FF // f_steps, D // 2 // o_steps
    out_at = lambda f: jnp.maximum(f - f_steps, 0)
    return pl.pallas_call(
        expert_kernel,
        grid=(f_steps + o_steps,),
        in_specs=[whole()] * 3 + [pl.BlockSpec(memory_space=pl.ANY)],
        out_specs=pl.BlockSpec((experts, 8, lanes), lambda f: (0, 0, out_at(f))),
        out_shape=sds((experts, 8, D // 2), BF),
        scratch_shapes=[
            pltpu.VMEM((experts * CAP, D), BF),
            pltpu.VMEM((f_steps, experts * CAP, fb), BF),
            pltpu.VMEM((FF, D), BF),
            pltpu.SemaphoreType.DMA((1,)),
        ],
        compiler_params=params(40),
        name="experts",
    )(
        in_vmem(slot_rows),
        in_vmem(gate),
        in_vmem(up),
        in_hbm(down),
    )


def run_combine(rows, bcol, wcol, mixed, per):
    toks = mixed.shape[0]
    n_rows = rows.shape[0]
    return pl.pallas_call(
        combine_kernel,
        grid=(2 * per,),
        in_specs=[
            whole(),
            full(toks, TOPK),
            full(toks, TOPK),
            pl.BlockSpec((toks, D // 2 // per), lambda n: (0, n)),
        ],
        out_specs=pl.BlockSpec((toks, D // 2 // per), lambda n: (0, n)),
        out_shape=jax.ShapeDtypeStruct((toks, D), BF),
        scratch_shapes=[pltpu.VMEM((TOPK * toks, n_rows), BF)],
        compiler_params=params(40),
        name="combine",
    )(in_vmem(rows), bcol, wcol, mixed)


def local(
    queries, kv_latent, rope_key, latent_norm_gain, key_up_weight, value_up_weight, out_proj,
    residual, ffn_gain, routes, route_weights, expert_gate, expert_up, expert_down,
):
    toks = queries.shape[1]
    sp = lax.axis_size("sp")
    experts = sp * lax.axis_size("dp")
    sds = jax.ShapeDtypeStruct
    offset = lax.axis_index("sp").astype(jnp.int32)[None]
    packed, ct, st = pl.pallas_call(
        prep_kernel,
        in_specs=[pl.BlockSpec(memory_space=pltpu.SMEM)] + [pl.BlockSpec()] * 4,
        out_shape=(sds((sp, LAT + ROT, toks), BF), sds((ROT, toks), F32), sds((ROT, toks), F32)),
        compiler_params=params(),
        name="prep",
    )(offset, kv_latent[0], rope_key[0].T, latent_norm_gain[None], pair_frequencies())
    keys = in_vmem(lax.all_to_all(packed, "sp", 0, 0, tiled=True))
    bcol, brow, wcol = pl.pallas_call(
        route_kernel,
        out_shape=(
            sds((toks, TOPK), jnp.int32), sds((TOPK, toks), jnp.int32), sds((toks, TOPK), F32)
        ),
        compiler_params=params(),
        name="routes",
    )(routes[0], routes[0].T, route_weights[0])

    mixed, normed, outgoing = attend(
        ready_queries(queries[0], ct, st, key_up_weight), keys, value_up_weight.T, out_proj,
        in_hbm(residual[0]), ffn_gain[None], brow, experts,
    )

    slot_rows = lax.all_to_all(
        outgoing.reshape(experts, 8, D // 2), ("sp", "dp"), 0, 0, tiled=True
    )
    expert_out = run_experts(
        slot_rows, expert_gate[0], expert_up[0], expert_down[0], F_STEPS, O_STEPS
    )
    returned = lax.all_to_all(expert_out, ("sp", "dp"), 0, 0, tiled=True)
    layer_out = run_combine(returned.reshape(experts * 8, D // 2), bcol, wcol, mixed, PER)
    return normed[None], layer_out[None]


def solution(mesh):
    tok = P("dp", "sp", None)
    exp = P(("sp", "dp"), None, None)
    in_specs = (
        tok, tok, tok, P(), P(), P(), P(), tok, P(), tok, tok, exp, exp, exp,
    )
    return jax.shard_map(
        local, mesh=mesh, in_specs=in_specs, out_specs=(tok, tok), check_vma=False
    )
```
